256 devices in a mesh: ep: 64 (over z, y, core), tp: 4 (over x).
Axes of the slice: x: 4, y: 4, z: 8, core: 2. Of those that a mesh axis runs over, the one named last changes fastest.
Arguments:
- queries: bfloat16 [16384, 2048], P('ep', 'tp'), may hold values from -150 to 150, as said below
- keys: bfloat16 [16384, 512], P('ep', 'tp'), may hold values from -6 to 6
- values: bfloat16 [16384, 512], P('ep', 'tp'), may hold values from -6 to 6
- cum_gates: float32 [16384, 16], P('ep', 'tp'), may hold values from -16384 to 0, as said below
- out_proj: bfloat16 [2048, 4096], P('tp'), may hold values from -0.125 to 0.125
- tokens: bfloat16 [8192, 4096], P('ep'), may hold values from -6 to 6
- norm_gain: float32 [4096], replicated, may hold values from 0.1 to 1.9
- routes: int32 [8192, 4], P('ep'), may hold values from 0 to 63, all different within a row; in each aligned block of 128 rows (0 to 127, 128 to 255, ...) at most 16 rows name the same one
- route_weights: float32 [8192, 4], P('ep'), may hold values from 0.2 to 1
- w_gate: bfloat16 [64, 4096, 1024], P('ep', None, 'tp'), may hold values from -0.09375 to 0.09375
- w_up: bfloat16 [64, 4096, 1024], P('ep', None, 'tp'), may hold values from -0.09375 to 0.09375
- w_down: bfloat16 [64, 1024, 4096], P('ep', 'tp'), may hold values from -0.1875 to 0.1875
Outputs:
- attn_mixed: bfloat16 [16384, 4096], P(('ep', 'tp'))
- moe_out: bfloat16 [8192, 4096], P('ep', 'tp')
The draws below stay inside these ranges and needn't reach their ends.
Inputs may be any that keep to these rules, and one draw needn't show every extreme that they name: keys and queries are of order one except where the draw sets a few queries far larger. `cum_gates`: never rises along positions. `routes`: each row names 4 different experts; among the rows of one index of ep no expert is named by more than 16 rows, a bound that some block reaches in some of them.
All inputs are finite; a program needn't handle non-finite values.
Results may differ from the reference program's by a relative error of at most 0.0109.
Values may be sent and summed in bfloat16 or wider, within the bound.
A program may use at most 128 MiB of HBM per device.

```python
import math
import jax
import jax.numpy as jnp
import numpy as np
from jax import lax

D = 4096
QH = 16
KVH = 4
HD = 128
DE = 1024
TOPK = 4
A_TOK = 256
E_TOK = 128
CONTEXT_SPAN = 16384
EXPERTS = 64
CAP = 16
N_EP = 64
N_TP = 4


def drawn_pair(key):
    query_base = jnp.clip(jax.random.normal(jax.random.fold_in(key, 11), (CONTEXT_SPAN, QH * HD), jnp.float32), -5.0, 5.0)
    key_base = jnp.clip(jax.random.normal(jax.random.fold_in(key, 12), (CONTEXT_SPAN, KVH * HD), jnp.float32), -5.0, 5.0)
    return (query_base, key_base)


def draw_queries(key, part):
    return drawn_pair(key)[0].astype(jnp.bfloat16)


def draw_keys(key, part):
    return drawn_pair(key)[1].astype(jnp.bfloat16)


def draw_cum_gates(key, part):
    order = jax.random.permutation(jax.random.fold_in(key, 21), QH)
    fast_count = QH // 2
    rapid_fading = (order < fast_count).astype(jnp.float32)
    fast_rate = jnp.exp(jax.random.uniform(jax.random.fold_in(key, 22), (QH,), jnp.float32, math.log(1.0 / 60.0), math.log(1.0 / 20.0)))
    slow_rate = jnp.exp(jax.random.uniform(jax.random.fold_in(key, 23), (QH,), jnp.float32, math.log(0.2), math.log(0.8))) / CONTEXT_SPAN
    rate = rapid_fading * fast_rate + (1.0 - rapid_fading) * slow_rate
    block_factor = jnp.exp(jax.random.uniform(jax.random.fold_in(key, 24), (CONTEXT_SPAN // A_TOK,), jnp.float32, math.log(0.5), math.log(2.0)))
    factor = jnp.repeat(block_factor, A_TOK)
    rough = jax.random.uniform(jax.random.fold_in(key, 25), (CONTEXT_SPAN, QH), jnp.float32, 0.2, 1.8)
    retention_logit = -rate[None, :] * factor[:, None] * rough
    flagged_indices = jax.random.randint(jax.random.fold_in(key, 26), (3,), 0, CONTEXT_SPAN)
    spike_occasions = jnp.zeros((CONTEXT_SPAN,), jnp.float32).at[flagged_indices].add(1.0)
    discarded_items = jnp.log(jax.random.uniform(jax.random.fold_in(key, 27), (QH,), jnp.float32, 0.55, 0.8))
    retention_logit = retention_logit + spike_occasions[:, None] * discarded_items[None, :] * (1.0 - rapid_fading)[None, :]
    return jnp.cumsum(retention_logit, axis=0)


def shard_levels(rng, extent, cuts, least, top_value):
    def one(dim, shards_of):
        steps = jax.random.uniform(jax.random.fold_in(jax.random.fold_in(rng, 6), dim), (shards_of,), jnp.float32, least / len(cuts), top_value / len(cuts))
        return jnp.repeat(jnp.exp(steps), extent[dim] // shards_of).reshape((-1,) + (1,) * (len(extent) - dim - 1))

    level = one(*cuts[0])
    for cut in cuts[1:]:
        level = level * one(*cut)
    return level


def assign_block(own_key, own, number, rows, number_of, top, bound, slope):
    sequence = jax.random.permutation(own_key, number_of)
    crowded, ordinary = load_shares(number_of, rows * top, bound, slope, True), load_shares(number_of, rows * top, bound, slope, False)
    places = jnp.arange(number_of)

    def named(tallies, rotation):
        used = int((tallies > 0).sum())
        fixed = max(1, used // 4)
        shifted = fixed + (places - fixed + rotation * (used - fixed)) % max(1, number_of - fixed)
        return jnp.zeros((number_of,), jnp.int32).at[sequence[jnp.where(places < fixed, places, shifted)]].set(jnp.asarray(tallies, jnp.int32))

    tallies = jnp.where(number % 4 == 0, named(crowded, number // 4), named(ordinary, number - number // 4 - 1))
    mixed = jax.random.permutation(jax.random.fold_in(own, 3), number_of)
    donor, taker = mixed[0:number_of // 2 * 2:2], mixed[1:number_of // 2 * 2:2]
    slack = jnp.minimum(tallies[donor] - 1, bound - tallies[taker]) // 2
    slack = jnp.where((donor == sequence[0]) | (taker == sequence[0]) | (tallies[taker] == 0), 0, jnp.maximum(slack, 0))
    shifted = jax.random.randint(jax.random.fold_in(own, 4), (number_of // 2,), 0, 1 << 20) % (slack + 1)
    tallies = tallies.at[donor].add(-shifted).at[taker].add(shifted)
    labels = jnp.searchsorted(jnp.cumsum(tallies), jnp.arange(rows * top), side="right").astype(jnp.int32)
    table = labels.reshape(top, rows).T
    table = table[jax.random.permutation(jax.random.fold_in(own, 1), rows)]
    rotation = jax.random.randint(jax.random.fold_in(own, 2), (rows, 1), 0, top)
    return jnp.take_along_axis(table, (jnp.arange(top)[None, :] + rotation) % top, axis=1)


def load_shares(amount, total, most, skew, full):
    loads = [(1 << 20) // math.isqrt(grade ** skew) + 1 for grade in range(1, amount + 1)]
    largest = most if full else min(most, max(-(-total // amount), total * loads[0] // sum(loads)))
    least = 1 if total - largest >= amount - 1 else 0
    holding, surplus = [largest] + [least] * (amount - 1), total - largest - least * (amount - 1)
    while surplus > 0:
        movable = [i for i in range(1, amount) if holding[i] < largest] or [i for i in range(1, amount) if holding[i] < most]
        whole, left = sum([loads[i] for i in movable]), surplus
        for i in movable:
            extra = min(most - holding[i], max(1, left * loads[i] // whole), surplus)
            holding[i] = holding[i] + extra
            surplus = surplus - extra
    return np.array(holding)


def scatter_about(own_key, dims, deviation, limit, pieces=(), kind=jnp.bfloat16):
    drawn = deviation * jax.random.normal(own_key, dims, jnp.float32)
    if pieces:
        drawn = drawn * shard_levels(own_key, dims, pieces, -0.22, 0.18)
    return jnp.clip(drawn, -limit, limit).astype(kind)


def setup_inputs(seed: int = 0) -> dict:
    arg_keys = jax.random.split(jax.random.key(seed), 13)
    queries = draw_queries(jax.random.fold_in(arg_keys[12], 71), 0)
    keys = draw_keys(jax.random.fold_in(arg_keys[12], 71), 0)
    values = scatter_about(arg_keys[2], (CONTEXT_SPAN, KVH * HD), 1.0, 6.0, ((0, 64), (1, 4)))
    cum_gates = draw_cum_gates(jax.random.fold_in(arg_keys[12], 71), 0)
    out_proj = scatter_about(arg_keys[4], (QH * HD, D), (QH * HD) ** -0.5, 0.125, ((0, 4),))
    tokens = scatter_about(arg_keys[5], (E_TOK * N_EP, D), 1.0, 6.0, ((0, 64),))
    norm_gain = jnp.clip(1.0 + 0.18 * jax.random.normal(arg_keys[6], (D,), jnp.float32), 0.1, 1.9)
    routes_keys = jax.random.split(jax.random.fold_in(arg_keys[7], 1), (E_TOK * N_EP) // E_TOK)
    routes_turns = jax.random.permutation(jax.random.fold_in(arg_keys[7], 3), (E_TOK * N_EP) // E_TOK)
    routes = jax.vmap(lambda own, number: assign_block(jax.random.fold_in(arg_keys[7], 2), own, number, E_TOK, EXPERTS, TOPK, CAP, 1))(routes_keys, routes_turns).reshape((E_TOK * N_EP, TOPK))
    route_weights = jnp.clip(0.2 + 0.8 * jax.random.uniform(arg_keys[8], (E_TOK * N_EP, TOPK), jnp.float32) ** shard_levels(arg_keys[8], (E_TOK * N_EP, TOPK), ((0, 64),), -0.2, 0.2), 0.2, 1.0)
    w_gate = scatter_about(arg_keys[9], (EXPERTS, D, DE), D ** -0.5, 0.09375, ((0, 64), (2, 4)))
    w_up = scatter_about(arg_keys[10], (EXPERTS, D, DE), D ** -0.5, 0.09375, ((0, 64), (2, 4)))
    w_down = scatter_about(arg_keys[11], (EXPERTS, DE, D), DE ** -0.5, 0.1875, ((0, 64), (1, 4)))
    return {"queries": queries, "keys": keys, "values": values, "cum_gates": cum_gates, "out_proj": out_proj, "tokens": tokens, "norm_gain": norm_gain, "routes": routes, "route_weights": route_weights, "w_gate": w_gate, "w_up": w_up, "w_down": w_down}


def attention_part(queries, keys, values, cum_gates, out_proj):
    group_ratio = QH // KVH
    score_scale = HD ** (-0.5)
    query_wide = queries.astype(jnp.float32).reshape(CONTEXT_SPAN, QH, HD)
    key_wide = jnp.repeat(keys.astype(jnp.float32).reshape(CONTEXT_SPAN, KVH, HD), group_ratio, axis=1)
    value_wide = jnp.repeat(values.astype(jnp.float32).reshape(CONTEXT_SPAN, KVH, HD), group_ratio, axis=1)
    gate_heads = cum_gates.T
    block_len = math.gcd(CONTEXT_SPAN, 512)
    outputs = []
    for block_index in range(CONTEXT_SPAN // block_len):
        row_begin = block_index * block_len
        row_end = row_begin + block_len
        scores = jnp.einsum('qhd,khd->hqk', query_wide[row_begin:row_end], key_wide[:row_end]) * score_scale
        scores = scores + gate_heads[:, row_begin:row_end, None] - gate_heads[:, None, :row_end]
        query_pos = row_begin + jnp.arange(block_len, dtype=jnp.int32)
        key_pos = jnp.arange(row_end, dtype=jnp.int32)
        allowed = key_pos[None, :] <= query_pos[:, None]
        scores = jnp.where(allowed[None], scores, -jnp.inf)
        largest = lax.optimization_barrier(jnp.max(scores, axis=-1, keepdims=True))
        weights = jnp.exp(scores - largest)
        totals = lax.optimization_barrier(jnp.sum(weights, axis=-1))
        rounded = lax.optimization_barrier(weights.astype(jnp.bfloat16)).astype(jnp.float32)
        weighted = jnp.einsum('hqk,khd->qhd', rounded, value_wide[:row_end])
        outputs.append((weighted / totals.T[:, :, None]).astype(jnp.bfloat16))
    heads_out = jnp.concatenate(outputs, axis=0).reshape(CONTEXT_SPAN, QH * HD)
    group_width = QH * HD // N_TP
    summed = jnp.zeros((CONTEXT_SPAN, D), jnp.float32)
    for part_index in range(N_TP):
        column_first = part_index * group_width
        col_end = column_first + group_width
        partial_value = jnp.dot(heads_out[:, column_first:col_end], out_proj[column_first:col_end], preferred_element_type=jnp.float32)
        summed = summed + lax.optimization_barrier(partial_value.astype(jnp.bfloat16)).astype(jnp.float32)
    return summed.astype(jnp.bfloat16)

def expert_portion(tokens, norm_gain, routes, route_weights, w_gate, w_up, w_down):
    tokens_wide = tokens.astype(jnp.float32)
    normed = (tokens_wide * lax.rsqrt(lax.optimization_barrier(jnp.mean(tokens_wide * tokens_wide, axis=-1, keepdims=True)) + 1e-06) * norm_gain.astype(jnp.float32)).astype(jnp.bfloat16)
    id_grid = routes.reshape(N_EP, E_TOK * TOPK)
    onehot = (id_grid[..., None] == jnp.arange(EXPERTS, dtype=jnp.int32)).astype(jnp.int32)
    slot_rank = lax.optimization_barrier(jnp.sum((jnp.cumsum(onehot, axis=1) - 1) * onehot, axis=2))
    source = jnp.arange(N_EP, dtype=jnp.int32)[:, None]
    position = source * CAP + slot_rank
    owner_row = source * E_TOK + jnp.arange(E_TOK * TOPK, dtype=jnp.int32)[None, :] // TOPK
    slot_rows = jnp.full((EXPERTS, N_EP * CAP), -1, jnp.int32)
    slot_rows = slot_rows.at[id_grid.reshape(-1), position.reshape(-1)].set(owner_row.reshape(-1))
    quarter = DE // N_TP

    def one_expert(packed):
        row_ids, gate_weight, up_weight, down_weight = packed
        filled = row_ids >= 0
        gathered = jnp.where(filled[:, None], normed[jnp.maximum(row_ids, 0)], jnp.zeros((), jnp.bfloat16))
        gate_act = jnp.dot(gathered, gate_weight, preferred_element_type=jnp.float32)
        up_act = jnp.dot(gathered, up_weight, preferred_element_type=jnp.float32)
        latent_width = (jax.nn.silu(gate_act) * up_act).astype(jnp.bfloat16)
        summed = jnp.zeros((row_ids.shape[0], D), jnp.float32)
        for part_index in range(N_TP):
            column_first = part_index * quarter
            partial_value = jnp.dot(latent_width[:, column_first:column_first + quarter], down_weight[column_first:column_first + quarter], preferred_element_type=jnp.float32)
            summed = summed + lax.optimization_barrier(partial_value.astype(jnp.bfloat16)).astype(jnp.float32)
        return summed.astype(jnp.bfloat16)
    results = lax.map(one_expert, (slot_rows, w_gate, w_up, w_down))
    picked = results[id_grid.reshape(-1), position.reshape(-1)].astype(jnp.float32).reshape(N_EP * E_TOK, TOPK, D)
    return lax.optimization_barrier(jnp.sum(picked * route_weights[:, :, None], axis=1)).astype(jnp.bfloat16)

def reference(queries, keys, values, cum_gates, out_proj, tokens, norm_gain, routes, route_weights, w_gate, w_up, w_down):
    attn_mixed = attention_part(queries, keys, values, cum_gates, out_proj)
    moe_out = expert_portion(tokens, norm_gain, routes, route_weights, w_gate, w_up, w_down)
    return (attn_mixed, moe_out)
```

```python
import functools
import math

import jax
import jax.numpy as jnp
from jax import lax
from jax.experimental import pallas as pl
from jax.experimental.pallas import tpu as pltpu
from jax.sharding import PartitionSpec as P

HD = 128
CAP = 16
NYC = 8
LOG2E = math.log2(math.e)
MESH = pl.DeviceIdType.MESH
F32 = jnp.float32
BF16 = jnp.bfloat16
FLOOR = -1e30


def iota(shape, dim):
    return lax.broadcasted_iota(jnp.int32, shape, dim)


def dot(a, b):
    return jnp.dot(a, b, preferred_element_type=F32)


def experts_kernel(
    nz, nk, nx,
    tok_ref, gain_ref, routes_ref, routes_t_ref, rw_ref, wg_hbm, wu_hbm, wd_hbm,
    o_ref,
    wg, wu, wd, out, arr, part, half_in, quart_in, res, ret, c_hi, c_lo,
    w_sem, a2a_send, a2a_recv, ag_send, ag_recv, fw_send, fw_recv,
    hs_send, hs_recv, qa_send, qa_recv, qb_send, qb_recv, ret_send, ret_recv,
):
    e = lax.axis_index("ep")
    x = lax.axis_index("tp")
    n_ep = nz * nk
    z, k_own = e // nk, e % nk
    right, left, far = (x + 1) % nx, (x + nx - 1) % nx, (x + 2) % nx
    rows, width = tok_ref.shape
    quarter = width // nx
    chunk_rows = nk * CAP
    half = chunk_rows // 2

    barrier = pltpu.get_barrier_semaphore()

    @pl.loop(1, n_ep)
    def _(k):
        pl.semaphore_signal(barrier, inc=1, device_id=((e + k) % n_ep, x), device_id_type=MESH)

    for side in (left, right):
        pl.semaphore_signal(barrier, inc=1, device_id=(e, side), device_id_type=MESH)

    loads = [
        pltpu.make_async_copy(src, dst, w_sem.at[i])
        for i, (src, dst) in enumerate(((wg_hbm, wg), (wu_hbm, wu), (wd_hbm, wd)))
    ]
    for load in loads:
        load.start()

    rt = routes_t_ref[...]
    e_row = iota((n_ep, rows), 0)
    named = jnp.zeros((n_ep, rows), F32)
    for k in range(rt.shape[0]):
        named = named + (rt[k : k + 1, :] == e_row).astype(F32)
    before = (iota((rows, rows), 0) < iota((rows, rows), 1)).astype(BF16)
    named = named.astype(BF16)
    rank = dot(named, before).astype(BF16)

    tokens = tok_ref[...].astype(F32)
    inv = lax.rsqrt(jnp.mean(tokens * tokens, axis=-1, keepdims=True) + 1e-06)
    mine = pl.ds(pl.multiple_of(x * quarter, quarter), quarter)
    normed = (tok_ref[:, mine].astype(F32) * inv * gain_ref[:, mine]).astype(BF16)

    @pl.loop(0, nz)
    def _(block):
        base = block * chunk_rows
        slot = iota((chunk_rows, n_ep), 0) + base
        spread = ((slot // CAP) == iota((chunk_rows, n_ep), 1)).astype(BF16)
        hit = (dot(spread, named) > 0.5) & (
            dot(spread, rank) == ((iota((chunk_rows, rows), 0) + base) % CAP).astype(F32)
        )
        at = pl.ds(pl.multiple_of(base, chunk_rows), chunk_rows)
        out[at, :] = dot(hit.astype(BF16), normed).astype(BF16)

    pl.semaphore_wait(barrier, n_ep - 1 + 2)

    def dz_of(c):
        return jnp.where(c % 2 == 1, (c + 1) // 2, (nz - c // 2) % nz)

    def slot_rows(index):
        return pl.ds(pl.multiple_of(index * CAP, CAP), CAP)

    @pl.loop(0, nz)
    def _(c):
        dest_z = (z + dz_of(c)) % nz

        @pl.loop(jnp.where(c == 0, 1, 0), nk)
        def _(k):
            dest = dest_z * nk + (k_own + k) % nk
            pltpu.make_async_remote_copy(
                out.at[slot_rows(dest)],
                arr.at[x, c, slot_rows(k_own)],
                a2a_send.at[c],
                a2a_recv.at[c],
                device_id=(dest, x),
                device_id_type=MESH,
            ).start()

    arr[x, 0, slot_rows(k_own), :] = out[slot_rows(e), :]

    routes = routes_ref[...]
    e_col = iota((rows, n_ep), 1)
    named2 = jnp.zeros((rows, n_ep), F32)
    weight = jnp.zeros((rows, n_ep), F32)
    for k in range(routes.shape[1]):
        hit = routes[:, k : k + 1] == e_col
        named2 = named2 + hit.astype(F32)
        weight = weight + jnp.where(hit, rw_ref[:, k : k + 1], 0.0)
    named2 = named2.astype(BF16)
    earlier = (iota((rows, rows), 1) < iota((rows, rows), 0)).astype(BF16)
    rank2 = dot(earlier, named2).astype(BF16)
    w_hi = weight.astype(BF16)
    w_lo = (weight - w_hi.astype(F32)).astype(BF16)

    slot = iota((n_ep, n_ep * CAP), 1)
    spread = ((slot // CAP) == iota((n_ep, n_ep * CAP), 0)).astype(BF16)
    keep = (dot(named2, spread) > 0.5) & (
        dot(rank2, spread) == (iota((rows, n_ep * CAP), 1) % CAP).astype(F32)
    )
    c_hi[...] = jnp.where(keep, dot(w_hi, spread), 0.0).astype(BF16)
    c_lo[...] = jnp.where(keep, dot(w_lo, spread), 0.0).astype(BF16)

    def await_bytes(ref, sem):
        pltpu.make_async_copy(ref, ref, sem).wait()

    def send(src, dst, send_sem, recv_sem, to):
        pltpu.make_async_remote_copy(
            src, dst, send_sem, recv_sem, device_id=(e, to), device_id_type=MESH
        ).start()

    low, high = pl.ds(0, half), pl.ds(half, half)
    first_rows = pl.ds(0, (nk - 1) * CAP)

    @pl.loop(0, nz + 4)
    def _(step):
        @pl.when(step < nz)
        def _():
            c = step

            @pl.when(c == 0)
            def _():
                await_bytes(arr.at[x, 0, first_rows], a2a_recv.at[0])

            @pl.when(c > 0)
            def _():
                await_bytes(arr.at[x, c], a2a_recv.at[c])

            send(arr.at[x, c], arr.at[x, c], ag_send.at[0, c], ag_recv.at[0, c], right)
            send(arr.at[x, c], arr.at[x, c], ag_send.at[1, c], ag_recv.at[1, c], left)

        @pl.when((step >= 1) & (step < nz + 1))
        def _():
            c = step - 1
            await_bytes(arr.at[left, c], ag_recv.at[0, c])
            send(arr.at[left, c, low], arr.at[left, c, low], fw_send.at[0, c], fw_recv.at[0, c], right)
            await_bytes(arr.at[right, c], ag_recv.at[1, c])
            send(arr.at[right, c, high], arr.at[right, c, high], fw_send.at[1, c], fw_recv.at[1, c], left)

        @pl.when(step == 2)
        def _():
            for load in loads:
                load.wait()

        @pl.when((step >= 2) & (step < nz + 2))
        def _():
            c = step - 2
            await_bytes(arr.at[far, c, low], fw_recv.at[0, c])
            await_bytes(arr.at[far, c, high], fw_recv.at[1, c])
            gate = jnp.zeros((chunk_rows, wg.shape[1]), F32)
            up = jnp.zeros((chunk_rows, wg.shape[1]), F32)
            for q in range(nx):
                rows_q = arr[q, c]
                gate = gate + dot(rows_q, wg[q * quarter : (q + 1) * quarter, :])
                up = up + dot(rows_q, wu[q * quarter : (q + 1) * quarter, :])
            hidden = (gate * jax.nn.sigmoid(gate) * up).astype(BF16)
            for q in range(nx):
                part[q, c] = dot(hidden, wd[:, q * quarter : (q + 1) * quarter]).astype(BF16)
            send(part.at[far, c, low], half_in.at[0, c], hs_send.at[0, c], hs_recv.at[0, c], right)
            send(part.at[far, c, high], half_in.at[1, c], hs_send.at[1, c], hs_recv.at[1, c], left)
            send(part.at[right, c, high], quart_in.at[0, c, high], qa_send.at[0, c], qa_recv.at[0, c], right)
            send(part.at[left, c, low], quart_in.at[1, c, low], qa_send.at[1, c], qa_recv.at[1, c], left)

        @pl.when((step >= 3) & (step < nz + 3))
        def _():
            c = step - 3
            await_bytes(half_in.at[0, c], hs_recv.at[0, c])
            part[right, c, 0:half, :] = (
                part[right, c, 0:half, :].astype(F32) + half_in[0, c].astype(F32)
            ).astype(BF16)
            send(part.at[right, c, low], quart_in.at[0, c, low], qb_send.at[0, c], qb_recv.at[0, c], right)
            await_bytes(half_in.at[1, c], hs_recv.at[1, c])
            part[left, c, half:, :] = (
                part[left, c, half:, :].astype(F32) + half_in[1, c].astype(F32)
            ).astype(BF16)
            send(part.at[left, c, high], quart_in.at[1, c, high], qb_send.at[1, c], qb_recv.at[1, c], left)

        @pl.when(step >= 4)
        def _():
            c = step - 4
            await_bytes(quart_in.at[0, c, high], qa_recv.at[0, c])
            await_bytes(quart_in.at[1, c, low], qa_recv.at[1, c])
            await_bytes(quart_in.at[0, c, low], qb_recv.at[0, c])
            await_bytes(quart_in.at[1, c, high], qb_recv.at[1, c])
            res[c] = (
                part[x, c].astype(F32) + quart_in[0, c].astype(F32) + quart_in[1, c].astype(F32)
            ).astype(BF16)
            home_z = (z + nz - dz_of(c)) % nz

            @pl.loop(jnp.where(c == 0, 1, 0), nk)
            def _(k):
                k_home = (k_own + k) % nk
                pltpu.make_async_remote_copy(
                    res.at[c, slot_rows(k_home)],
                    ret.at[slot_rows(e)],
                    ret_send.at[c],
                    ret_recv,
                    device_id=(home_z * nk + k_home, x),
                    device_id_type=MESH,
                ).start()

    ret[slot_rows(e), :] = res[0, slot_rows(k_own), :]
    await_bytes(ret.at[pl.ds(0, (n_ep - 1) * CAP)], ret_recv)
    o_ref[...] = (dot(c_hi[...], ret[...]) + dot(c_lo[...], ret[...])).astype(BF16)

    await_bytes(res.at[0, first_rows], ret_send.at[0])
    await_bytes(arr.at[0, 0, first_rows], a2a_send.at[0])

    @pl.loop(1, nz)
    def _(c):
        await_bytes(res.at[c], ret_send.at[c])
        await_bytes(arr.at[0, c], a2a_send.at[c])

    @pl.loop(0, nz)
    def _(c):
        for side in (0, 1):
            await_bytes(arr.at[0, c], ag_send.at[side, c])
            for sem in (fw_send, hs_send, qa_send, qb_send):
                await_bytes(half_in.at[side, c], sem.at[side, c])


def experts_part(tokens, norm_gain, routes, route_weights, w_gate, w_up, w_down):
    rows, width = tokens.shape
    n_ep, nx = lax.axis_size("ep"), lax.axis_size("tp")
    nk = NYC
    nz = n_ep // nk
    quarter = width // nx
    hidden = w_gate.shape[2]
    chunk = nk * CAP
    slots = n_ep * CAP
    vmem = pl.BlockSpec(memory_space=pltpu.VMEM)
    anywhere = pl.BlockSpec(memory_space=pl.ANY)
    dma = pltpu.SemaphoreType.DMA
    pair = dma((2, nz))
    return pl.pallas_call(
        functools.partial(experts_kernel, nz, nk, nx),
        out_shape=jax.ShapeDtypeStruct((rows, quarter), BF16),
        in_specs=[vmem] * 5 + [anywhere] * 3,
        out_specs=vmem,
        scratch_shapes=[
            pltpu.VMEM((width, hidden), BF16),
            pltpu.VMEM((width, hidden), BF16),
            pltpu.VMEM((hidden, width), BF16),
            pltpu.VMEM((slots, quarter), BF16),
            pltpu.VMEM((nx, nz, chunk, quarter), BF16),
            pltpu.VMEM((nx, nz, chunk, quarter), BF16),
            pltpu.VMEM((2, nz, chunk // 2, quarter), BF16),
            pltpu.VMEM((2, nz, chunk, quarter), BF16),
            pltpu.VMEM((nz, chunk, quarter), BF16),
            pltpu.VMEM((slots, quarter), BF16),
            pltpu.VMEM((rows, slots), BF16),
            pltpu.VMEM((rows, slots), BF16),
            dma((3,)),
            dma((nz,)),
            dma((nz,)),
            pair, pair, pair, pair, pair, pair, pair, pair, pair, pair,
            dma((nz,)),
            dma,
        ],
        compiler_params=pltpu.CompilerParams(
            collective_id=0, has_side_effects=True, vmem_limit_bytes=58 * 2**20
        ),
        cost_estimate=pl.CostEstimate(
            flops=100 * 10**9, bytes_accessed=10 * 2**20, transcendentals=0
        ),
    )(
        tokens,
        norm_gain[None],
        routes,
        routes.T,
        route_weights,
        w_gate[0],
        w_up[0],
        w_down[0],
    )


def flash_kernel(q_ref, kvg_ref, own_ref, o_ref, m_ref, l_ref, acc_ref):
    e = lax.axis_index("ep")
    rows = q_ref.shape[0]
    heads = q_ref.shape[1] // HD
    m_ref[...] = jnp.full_like(m_ref, FLOOR)
    l_ref[...] = jnp.zeros_like(l_ref)
    acc_ref[...] = jnp.zeros_like(acc_ref)
    halves = rows // 128
    ratio = HD ** (-0.5) * LOG2E
    base = own_ref[...][:, 0:1] * 1.0

    def visit(j, masked):
        key = kvg_ref[pl.ds(2 * j, 2), 0:rows, :].reshape(2 * rows, HD)
        value = kvg_ref[pl.ds(2 * j, 2), rows : 2 * rows, :].reshape(2 * rows, HD)
        pieces = kvg_ref[pl.ds(2 * j, 2), 2 * rows :, :].astype(F32)
        n = heads * halves
        gates = pieces[:, 0:n] + pieces[:, n : 2 * n] + pieces[:, 2 * n : 3 * n]
        if masked:
            pos = j * 2 * rows + iota((rows, 2 * rows), 1)
            own_pos = e * rows + iota((rows, 2 * rows), 0)
            allowed = pos <= own_pos
        for h in range(heads):
            line = jnp.concatenate(
                [gates[b, h * halves + i : h * halves + i + 1, :] for b in range(2) for i in range(halves)],
                axis=1,
            )
            line = (line - base[h * halves : h * halves + 1, :]) * LOG2E
            s = lax.dot_general(
                q_ref[:, h * HD : (h + 1) * HD], key, (((1,), (1,)), ((), ())), preferred_element_type=F32
            )
            t = s * ratio - line
            if masked:
                t = jnp.where(allowed, t, FLOOR)
            old = m_ref[h]
            new = jnp.maximum(old, jnp.max(t, axis=1, keepdims=True))
            alpha = jnp.exp2(old - new)
            w = jnp.exp2(t - new)
            l_ref[h] = alpha * l_ref[h] + jnp.sum(w, axis=1, keepdims=True)
            acc_ref[h] = alpha * acc_ref[h] + dot(w.astype(BF16), value)
            m_ref[h] = new

    @pl.loop(0, e // 2)
    def _(j):
        visit(j, False)

    visit(e // 2, True)
    for h in range(heads):
        o_ref[:, h * HD : (h + 1) * HD] = (acc_ref[h] / l_ref[h]).astype(BF16)


def attend(queries, keys, values, cum_gates, out_proj, experts):
    rows = queries.shape[0]
    heads = cum_gates.shape[1]
    lines = cum_gates.T.reshape(heads * rows // 128, 128)
    hi = lax.reduce_precision(lines, 8, 7)
    mid = lax.reduce_precision(lines - hi, 8, 7)
    lo = lines - hi - mid
    pieces = jnp.concatenate([hi, mid, lo], axis=0).astype(BF16)
    packed = jnp.concatenate([keys, values, pieces], axis=0)
    gathered = lax.all_gather(packed, "ep", axis=0, tiled=False)
    gathered, routed = lax.optimization_barrier((gathered, experts))
    vmem = pl.BlockSpec(memory_space=pltpu.VMEM)
    heads_out = pl.pallas_call(
        flash_kernel,
        out_shape=jax.ShapeDtypeStruct(queries.shape, BF16),
        in_specs=[vmem] * 3,
        out_specs=vmem,
        scratch_shapes=[
            pltpu.VMEM((heads, rows, 1), F32),
            pltpu.VMEM((heads, rows, 1), F32),
            pltpu.VMEM((heads, rows, HD), F32),
        ],
        compiler_params=pltpu.CompilerParams(vmem_limit_bytes=40 * 2**20),
        cost_estimate=pl.CostEstimate(
            flops=20 * 10**9, bytes_accessed=10 * 2**20, transcendentals=16 * 2**20
        ),
    )(queries, gathered, lines)
    mixed = lax.psum_scatter(
        jnp.dot(heads_out, out_proj, preferred_element_type=F32).astype(BF16),
        "tp",
        scatter_dimension=0,
        tiled=True,
    )
    return (mixed, routed)


def per_device(
    queries, keys, values, cum_gates, out_proj,
    tokens, norm_gain, routes, route_weights, w_gate, w_up, w_down,
):
    routed = experts_part(tokens, norm_gain, routes, route_weights, w_gate, w_up, w_down)
    return attend(queries, keys, values, cum_gates, out_proj, routed)


def solution(mesh):
    placed = (
        P("ep", "tp"), P("ep", "tp"), P("ep", "tp"), P("ep", "tp"), P("tp", None),
        P("ep", None), P(), P("ep", None), P("ep", None),
        P("ep", None, "tp"), P("ep", None, "tp"), P("ep", "tp", None),
    )
    return jax.shard_map(
        per_device,
        mesh=mesh,
        in_specs=placed,
        out_specs=(P(("ep", "tp"), None), P("ep", "tp")),
        check_vma=False,
    )
```

```python
import functools
import math

import jax
import jax.numpy as jnp
from jax import lax
from jax.experimental import pallas as pl
from jax.experimental.pallas import tpu as pltpu
from jax.sharding import PartitionSpec as P

HD = 128
CAP = 16
NYC = 8
LOG2E = math.log2(math.e)
MESH = pl.DeviceIdType.MESH
F32 = jnp.float32
BF16 = jnp.bfloat16
FLOOR = -1e30
AHEAD = 4


def iota(shape, dim):
    return lax.broadcasted_iota(jnp.int32, shape, dim)


def dot(a, b):
    return jnp.dot(a, b, preferred_element_type=F32)


def step_kernel(
    nz, nk, nx,
    tok_ref, gain_ref, routes_ref, routes_t_ref, rw_ref, q_ref, lines_ref,
    wg_hbm, wu_hbm, wd_hbm, wo_hbm, key_hbm, value_hbm,
    mixed_ref, o_ref,
    wg, wu, wd, wo, out, arr, part, half_in, quart_in, ret, c_hi, c_lo,
    kv, m_ref, l_ref, acc_ref, heads_ref,
    w_sem, a2a_send, a2a_recv, ag_send, ag_recv, fw_send, fw_recv,
    hs_send, hs_recv, qa_send, qa_recv, qb_send, qb_recv, ret_send, ret_recv,
    kz_send, kz_recv, ky_send, ky_recv, kf_send, kf_recv, ks_send, ks_recv,
):
    e = lax.axis_index("ep")
    x = lax.axis_index("tp")
    n_ep = nz * nk
    ny = nk // 2
    z, k_own = e // nk, e % nk
    y, core = k_own // 2, k_own % 2
    right, left, far = (x + 1) % nx, (x + nx - 1) % nx, (x + 2) % nx
    rows, width = tok_ref.shape
    quarter = width // nx
    chunk_rows = nk * CAP
    half = chunk_rows // 2
    q_rows = q_ref.shape[0]
    heads = q_ref.shape[1] // HD
    block_rows = kv.shape[2]

    barrier = pltpu.get_barrier_semaphore()

    @pl.loop(1, n_ep)
    def _(k):
        pl.semaphore_signal(barrier, inc=1, device_id=((e + k) % n_ep, x), device_id_type=MESH)

    for side in (left, right):
        pl.semaphore_signal(barrier, inc=1, device_id=(e, side), device_id_type=MESH)

    own_kv = [
        pltpu.make_async_copy(key_hbm, kv.at[z, k_own, pl.ds(0, q_rows)], w_sem.at[4]),
        pltpu.make_async_copy(value_hbm, kv.at[z, k_own, pl.ds(q_rows, q_rows)], w_sem.at[5]),
    ]
    loads = [
        pltpu.make_async_copy(src, dst, w_sem.at[i])
        for i, (src, dst) in enumerate(((wg_hbm, wg), (wu_hbm, wu), (wd_hbm, wd), (wo_hbm, wo)))
    ]
    for load in own_kv + loads:
        load.start()

    lines = lines_ref[...]
    g_hi = lines.astype(BF16)
    rest = lines - g_hi.astype(F32)
    g_mid = rest.astype(BF16)
    g_lo = (rest - g_mid.astype(F32)).astype(BF16)
    n_lines = lines.shape[0]
    kv[z, k_own, 2 * q_rows :, :] = jnp.concatenate(
        [g_hi.astype(F32), g_mid.astype(F32), g_lo.astype(F32), jnp.zeros_like(lines)], axis=0
    ).astype(BF16)

    rt = routes_t_ref[...]
    e_row = iota((n_ep, rows), 0)
    named = jnp.zeros((n_ep, rows), F32)
    for k in range(rt.shape[0]):
        named = named + (rt[k : k + 1, :] == e_row).astype(F32)
    before = (iota((rows, rows), 0) < iota((rows, rows), 1)).astype(BF16)
    named = named.astype(BF16)
    rank = dot(named, before).astype(BF16)

    tokens = tok_ref[...].astype(F32)
    inv = lax.rsqrt(jnp.mean(tokens * tokens, axis=-1, keepdims=True) + 1e-06)
    mine = pl.ds(pl.multiple_of(x * quarter, quarter), quarter)
    normed = (tok_ref[:, mine].astype(F32) * inv * gain_ref[:, mine]).astype(BF16)

    @pl.loop(0, nz)
    def _(block):
        base = block * chunk_rows
        slot = iota((chunk_rows, n_ep), 0) + base
        spread = ((slot // CAP) == iota((chunk_rows, n_ep), 1)).astype(BF16)
        hit = (dot(spread, named) > 0.5) & (
            dot(spread, rank) == ((iota((chunk_rows, rows), 0) + base) % CAP).astype(F32)
        )
        at = pl.ds(pl.multiple_of(base, chunk_rows), chunk_rows)
        out[at, :] = dot(hit.astype(BF16), normed).astype(BF16)

    for load in own_kv:
        load.wait()
    pl.semaphore_wait(barrier, n_ep - 1 + 2)

    def dz_of(c):
        return jnp.where(c % 2 == 1, (c + 1) // 2, (nz - c // 2) % nz)

    def slot_rows(index):
        return pl.ds(pl.multiple_of(index * CAP, CAP), CAP)

    def await_bytes(ref, sem):
        pltpu.make_async_copy(ref, ref, sem).wait()

    def send(src, dst, send_sem, recv_sem, to):
        pltpu.make_async_remote_copy(
            src, dst, send_sem, recv_sem, device_id=(e, to), device_id_type=MESH
        ).start()

    def send_block(ref, send_sem, recv_sem, to):
        pltpu.make_async_remote_copy(
            ref, ref, send_sem, recv_sem, device_id=(to, x), device_id_type=MESH
        ).start()

    def dispatch(c):
        dest_z = (z + dz_of(c)) % nz

        @pl.loop(jnp.where(c == 0, 1, 0), nk)
        def _(k):
            dest = dest_z * nk + (k_own + k) % nk
            pltpu.make_async_remote_copy(
                out.at[slot_rows(dest)],
                arr.at[x, c, slot_rows(k_own)],
                a2a_send.at[c],
                a2a_recv.at[c],
                device_id=(dest, x),
                device_id_type=MESH,
            ).start()

    ahead = min(AHEAD, nz)

    @pl.loop(0, ahead)
    def _(c):
        dispatch(c)

    arr[x, 0, slot_rows(k_own), :] = out[slot_rows(e), :]

    routes = routes_ref[...]
    e_col = iota((rows, n_ep), 1)
    named2 = jnp.zeros((rows, n_ep), F32)
    weight = jnp.zeros((rows, n_ep), F32)
    for k in range(routes.shape[1]):
        hit = routes[:, k : k + 1] == e_col
        named2 = named2 + hit.astype(F32)
        weight = weight + jnp.where(hit, rw_ref[:, k : k + 1], 0.0)
    named2 = named2.astype(BF16)
    earlier = (iota((rows, rows), 1) < iota((rows, rows), 0)).astype(BF16)
    rank2 = dot(earlier, named2).astype(BF16)
    w_hi = weight.astype(BF16)
    w_lo = (weight - w_hi.astype(F32)).astype(BF16)

    slot = iota((n_ep, n_ep * CAP), 1)
    spread = ((slot // CAP) == iota((n_ep, n_ep * CAP), 0)).astype(BF16)
    keep = (dot(named2, spread) > 0.5) & (
        dot(rank2, spread) == (iota((rows, n_ep * CAP), 1) % CAP).astype(F32)
    )
    c_hi[...] = jnp.where(keep, dot(w_hi, spread), 0.0).astype(BF16)
    c_lo[...] = jnp.where(keep, dot(w_lo, spread), 0.0).astype(BF16)

    m_ref[...] = jnp.full_like(m_ref, FLOOR)
    l_ref[...] = jnp.zeros_like(l_ref)
    acc_ref[...] = jnp.zeros_like(acc_ref)
    halves = q_rows // 128
    ratio = HD ** (-0.5) * LOG2E

    def visit(zs, p, masked):
        both = pl.ds(2 * p, 2)
        key = kv[zs, both, 0:q_rows, :].reshape(2 * q_rows, HD)
        value = kv[zs, both, q_rows : 2 * q_rows, :].reshape(2 * q_rows, HD)
        terms = kv[zs, both, 2 * q_rows :, :].astype(F32)
        n = n_lines
        gates = terms[:, 0:n] + terms[:, n : 2 * n] + terms[:, 2 * n : 3 * n]
        if masked:
            pos = p * 2 * q_rows + iota((q_rows, 2 * q_rows), 1)
            own_pos = k_own * q_rows + iota((q_rows, 2 * q_rows), 0)
            allowed = pos <= own_pos
        for h in range(heads):
            line = jnp.concatenate(
                [gates[b, h * halves + i : h * halves + i + 1, :] for b in range(2) for i in range(halves)],
                axis=1,
            )
            line = (line - lines_ref[h * halves : h * halves + 1, 0:1]) * LOG2E
            s = lax.dot_general(
                q_ref[:, h * HD : (h + 1) * HD], key, (((1,), (1,)), ((), ())), preferred_element_type=F32
            )
            t = s * ratio - line
            if masked:
                t = jnp.where(allowed, t, FLOOR)
            old = m_ref[h]
            new = jnp.maximum(old, jnp.max(t, axis=1, keepdims=True))
            alpha = jnp.exp2(old - new)
            w = jnp.exp2(t - new)
            l_ref[h] = alpha * l_ref[h] + jnp.sum(w, axis=1, keepdims=True)
            acc_ref[h] = alpha * acc_ref[h] + dot(w.astype(BF16), value)
            m_ref[h] = new

    low, high = pl.ds(0, half), pl.ds(half, half)
    first_rows = pl.ds(0, (nk - 1) * CAP)
    b_low, b_high = pl.ds(0, block_rows // 2), pl.ds(block_rows // 2, block_rows // 2)
    y_up, y_down, y_far = (y + 1) % ny, (y + ny - 1) % ny, (y + 2) % ny
    plane = z * nk
    up_dev, down_dev = plane + y_up * 2 + core, plane + y_down * 2 + core
    sibling = plane + y * 2 + (1 - core)

    def scatter_sends(c):
        send(part.at[far, c, low], half_in.at[0, c], hs_send.at[0, c], hs_recv.at[0, c], right)
        send(part.at[far, c, high], half_in.at[1, c], hs_send.at[1, c], hs_recv.at[1, c], left)
        send(part.at[right, c, high], quart_in.at[0, c, high], qa_send.at[0, c], qa_recv.at[0, c], right)
        send(part.at[left, c, low], quart_in.at[1, c, low], qa_send.at[1, c], qa_recv.at[1, c], left)

    @pl.loop(0, nz + 6)
    def _(step):
        @pl.when(step + ahead < nz)
        def _():
            dispatch(step + ahead)

        @pl.when(step < nz)
        def _():
            c = step

            @pl.when(c == 0)
            def _():
                await_bytes(arr.at[x, 0, first_rows], a2a_recv.at[0])

            @pl.when(c > 0)
            def _():
                await_bytes(arr.at[x, c], a2a_recv.at[c])

            send(arr.at[x, c], arr.at[x, c], ag_send.at[0, c], ag_recv.at[0, c], right)
            send(arr.at[x, c], arr.at[x, c], ag_send.at[1, c], ag_recv.at[1, c], left)

        @pl.when((step < nz) & (step <= z))
        def _():
            d = step
            block = kv.at[z - d, k_own]

            @pl.when(d > 0)
            def _():
                await_bytes(block, kz_recv.at[d])

            @pl.when(z + 1 < nz)
            def _():
                send_block(block, kz_send.at[d], kz_recv.at[d + 1], e + nk)

            send_block(block, ky_send.at[0, d], ky_recv.at[0, d], up_dev)
            send_block(block, ky_send.at[1, d], ky_recv.at[1, d], down_dev)
            send_block(block, ks_send.at[0, d], ks_recv.at[0, d], sibling)

        @pl.when((step >= 1) & (step < nz + 1))
        def _():
            c = step - 1
            await_bytes(arr.at[left, c], ag_recv.at[0, c])
            send(arr.at[left, c, low], arr.at[left, c, low], fw_send.at[0, c], fw_recv.at[0, c], right)
            await_bytes(arr.at[right, c], ag_recv.at[1, c])
            send(arr.at[right, c, high], arr.at[right, c, high], fw_send.at[1, c], fw_recv.at[1, c], left)

        @pl.when((step >= 1) & (step < nz + 1) & (step - 1 <= z))
        def _():
            d = step - 1
            zs = z - d
            below = kv.at[zs, y_down * 2 + core]
            await_bytes(below, ky_recv.at[0, d])
            part_low = kv.at[zs, y_down * 2 + core, b_low]
            send_block(part_low, kf_send.at[0, d], kf_recv.at[0, d], up_dev)
            send_block(below, ks_send.at[1, d], ks_recv.at[1, d], sibling)
            above = kv.at[zs, y_up * 2 + core]
            await_bytes(above, ky_recv.at[1, d])
            part_high = kv.at[zs, y_up * 2 + core, b_high]
            send_block(part_high, kf_send.at[1, d], kf_recv.at[1, d], down_dev)
            send_block(above, ks_send.at[2, d], ks_recv.at[2, d], sibling)

        @pl.when(step == 2)
        def _():
            for load in loads[:3]:
                load.wait()

        @pl.when((step >= 2) & (step < nz + 2))
        def _():
            c = step - 2
            await_bytes(arr.at[far, c, low], fw_recv.at[0, c])
            await_bytes(arr.at[far, c, high], fw_recv.at[1, c])
            gate = jnp.zeros((chunk_rows, wg.shape[1]), F32)
            up = jnp.zeros((chunk_rows, wg.shape[1]), F32)
            for q in range(nx):
                rows_q = arr[q, c]
                gate = gate + dot(rows_q, wg[q * quarter : (q + 1) * quarter, :])
                up = up + dot(rows_q, wu[q * quarter : (q + 1) * quarter, :])
            hidden = (gate * jax.nn.sigmoid(gate) * up).astype(BF16)
            for q in range(nx):
                part[q, c] = dot(hidden, wd[:, q * quarter : (q + 1) * quarter]).astype(BF16)
            scatter_sends(c)

        @pl.when((step >= 3) & (step < nz + 5))
        def _():
            c = step - 3
            await_bytes(half_in.at[0, c], hs_recv.at[0, c])
            part[right, c, 0:half, :] = (
                part[right, c, 0:half, :].astype(F32) + half_in[0, c].astype(F32)
            ).astype(BF16)
            send(part.at[right, c, low], quart_in.at[0, c, low], qb_send.at[0, c], qb_recv.at[0, c], right)
            await_bytes(half_in.at[1, c], hs_recv.at[1, c])
            part[left, c, half:, :] = (
                part[left, c, half:, :].astype(F32) + half_in[1, c].astype(F32)
            ).astype(BF16)
            send(part.at[left, c, high], quart_in.at[1, c, high], qb_send.at[1, c], qb_recv.at[1, c], left)

        @pl.when(step >= 4)
        def _():
            c = step - 4
            await_bytes(quart_in.at[0, c, high], qa_recv.at[0, c])
            await_bytes(quart_in.at[1, c, low], qa_recv.at[1, c])
            await_bytes(quart_in.at[0, c, low], qb_recv.at[0, c])
            await_bytes(quart_in.at[1, c, high], qb_recv.at[1, c])
            part[x, c] = (
                part[x, c].astype(F32) + quart_in[0, c].astype(F32) + quart_in[1, c].astype(F32)
            ).astype(BF16)

            @pl.when(c < nz)
            def _():
                home_z = (z + nz - dz_of(c)) % nz

                @pl.loop(jnp.where(c == 0, 1, 0), nk)
                def _(k):
                    k_home = (k_own + k) % nk
                    pltpu.make_async_remote_copy(
                        part.at[x, c, slot_rows(k_home)],
                        ret.at[slot_rows(e)],
                        ret_send.at[c],
                        ret_recv,
                        device_id=(home_z * nk + k_home, x),
                        device_id_type=MESH,
                    ).start()

        @pl.when((step >= 2) & (step < nz + 2) & (step - 2 <= z))
        def _():
            d = step - 2
            zs = z - d
            opposite = y_far * 2 + core
            await_bytes(kv.at[zs, opposite, b_low], kf_recv.at[0, d])
            await_bytes(kv.at[zs, opposite, b_high], kf_recv.at[1, d])
            send_block(kv.at[zs, opposite], ks_send.at[3, d], ks_recv.at[3, d], sibling)

        @pl.when((step >= 3) & (step < nz + 3) & (step - 3 <= z))
        def _():
            d = step - 3
            zs = z - d
            for i, line_y in enumerate((y, y_down, y_up, y_far)):
                await_bytes(kv.at[zs, line_y * 2 + 1 - core], ks_recv.at[i, d])

            @pl.loop(0, jnp.where(d == 0, k_own // 2, nk // 2))
            def _(p):
                visit(zs, p, False)

            @pl.when(d == 0)
            def _():
                visit(zs, k_own // 2, True)

        @pl.when(step == nz + 2)
        def _():
            loads[3].wait()
            for h in range(heads):
                heads_ref[:, h * HD : (h + 1) * HD] = (acc_ref[h] / l_ref[h]).astype(BF16)
            for n in range(nx):
                mixed = dot(heads_ref[...], wo[:, n * quarter : (n + 1) * quarter]).astype(BF16)
                for q in range(nx):
                    part[q, nz + n // 2, n % 2 * half : n % 2 * half + half, :] = mixed[
                        q * half : (q + 1) * half, :
                    ]
            scatter_sends(nz)
            scatter_sends(nz + 1)

    for n in range(nx):
        mixed_ref[:, n * quarter : (n + 1) * quarter] = part[
            x, nz + n // 2, n % 2 * half : n % 2 * half + half, :
        ]

    ret[slot_rows(e), :] = part[x, 0, slot_rows(k_own), :]
    await_bytes(ret.at[pl.ds(0, (n_ep - 1) * CAP)], ret_recv)
    o_ref[...] = (dot(c_hi[...], ret[...]) + dot(c_lo[...], ret[...])).astype(BF16)

    await_bytes(part.at[x, 0, first_rows], ret_send.at[0])
    await_bytes(arr.at[0, 0, first_rows], a2a_send.at[0])

    @pl.loop(1, nz)
    def _(c):
        await_bytes(part.at[x, c], ret_send.at[c])
        await_bytes(arr.at[0, c], a2a_send.at[c])

    @pl.loop(0, nz)
    def _(c):
        for side in (0, 1):
            await_bytes(arr.at[0, c], ag_send.at[side, c])
            await_bytes(half_in.at[side, c], fw_send.at[side, c])

        @pl.when(c <= z)
        def _():
            block = kv.at[0, 0]

            @pl.when(z + 1 < nz)
            def _():
                await_bytes(block, kz_send.at[c])

            for side in (0, 1):
                await_bytes(block, ky_send.at[side, c])
                await_bytes(kv.at[0, 0, b_low], kf_send.at[side, c])
            for i in range(4):
                await_bytes(block, ks_send.at[i, c])

    @pl.loop(0, nz + 2)
    def _(c):
        for side in (0, 1):
            for sem in (hs_send, qa_send, qb_send):
                await_bytes(half_in.at[side, c], sem.at[side, c])


def per_device(
    queries, keys, values, cum_gates, out_proj,
    tokens, norm_gain, routes, route_weights, w_gate, w_up, w_down,
):
    rows, width = tokens.shape
    q_rows = queries.shape[0]
    heads = cum_gates.shape[1]
    n_ep, nx = lax.axis_size("ep"), lax.axis_size("tp")
    nk = NYC
    nz = n_ep // nk
    quarter = width // nx
    hidden = w_gate.shape[2]
    chunk = nk * CAP
    slots = n_ep * CAP
    lines = cum_gates.T.reshape(heads * q_rows // 128, 128)
    block_rows = 2 * q_rows + 4 * lines.shape[0]
    vmem = pl.BlockSpec(memory_space=pltpu.VMEM)
    anywhere = pl.BlockSpec(memory_space=pl.ANY)
    dma = pltpu.SemaphoreType.DMA
    pair = dma((2, nz))
    more = dma((2, nz + 2))
    line = dma((nz + 1,))
    return pl.pallas_call(
        functools.partial(step_kernel, nz, nk, nx),
        out_shape=(
            jax.ShapeDtypeStruct((q_rows // nx, width), BF16),
            jax.ShapeDtypeStruct((rows, quarter), BF16),
        ),
        in_specs=[vmem] * 7 + [anywhere] * 6,
        out_specs=(vmem, vmem),
        scratch_shapes=[
            pltpu.VMEM((width, hidden), BF16),
            pltpu.VMEM((width, hidden), BF16),
            pltpu.VMEM((hidden, width), BF16),
            pltpu.VMEM(out_proj.shape, BF16),
            pltpu.VMEM((slots, quarter), BF16),
            pltpu.VMEM((nx, nz, chunk, quarter), BF16),
            pltpu.VMEM((nx, nz + 2, chunk, quarter), BF16),
            pltpu.VMEM((2, nz + 2, chunk // 2, quarter), BF16),
            pltpu.VMEM((2, nz + 2, chunk, quarter), BF16),
            pltpu.VMEM((slots, quarter), BF16),
            pltpu.VMEM((rows, slots), BF16),
            pltpu.VMEM((rows, slots), BF16),
            pltpu.VMEM((nz, nk, block_rows, HD), BF16),
            pltpu.VMEM((heads, q_rows, 1), F32),
            pltpu.VMEM((heads, q_rows, 1), F32),
            pltpu.VMEM((heads, q_rows, HD), F32),
            pltpu.VMEM((q_rows, heads * HD), BF16),
            dma((6,)),
            dma((nz,)), dma((nz,)),
            pair, pair, pair, pair,
            more, more, more, more, more, more,
            dma((nz,)),
            dma,
            line, line, pair, pair, pair, pair, dma((4, nz)), dma((4, nz)),
        ],
        compiler_params=pltpu.CompilerParams(
            collective_id=0, has_side_effects=True, vmem_limit_bytes=67043328
        ),
        cost_estimate=pl.CostEstimate(
            flops=100 * 10**9, bytes_accessed=10 * 2**20, transcendentals=0
        ),
    )(
        tokens, norm_gain[None], routes, routes.T, route_weights, queries, lines,
        w_gate[0], w_up[0], w_down[0], out_proj, keys, values,
    )


def solution(mesh):
    placed = (
        P("ep", "tp"), P("ep", "tp"), P("ep", "tp"), P("ep", "tp"), P("tp", None),
        P("ep", None), P(), P("ep", None), P("ep", None),
        P("ep", None, "tp"), P("ep", None, "tp"), P("ep", "tp", None),
    )
    return jax.shard_map(
        per_device,
        mesh=mesh,
        in_specs=placed,
        out_specs=(P(("ep", "tp"), None), P("ep", "tp")),
        check_vma=False,
    )
```

```python
import functools
import math

import jax
import jax.numpy as jnp
from jax import lax
from jax.experimental import pallas as pl
from jax.experimental.pallas import tpu as pltpu
from jax.sharding import PartitionSpec as P

HD = 128
CAP = 16
NYC = 8
LOG2E = math.log2(math.e)
MESH = pl.DeviceIdType.MESH
F32 = jnp.float32
BF16 = jnp.bfloat16
FLOOR = -1e30
AHEAD = 2


def iota(shape, dim):
    return lax.broadcasted_iota(jnp.int32, shape, dim)


def dot(a, b):
    return jnp.dot(a, b, preferred_element_type=F32)


def step_kernel(
    nz, nk, nx,
    tok_ref, gain_ref, routes_ref, routes_t_ref, rw_ref, q_ref, lines_ref,
    wg_hbm, wu_hbm, wd_hbm, wo_hbm, key_hbm, value_hbm,
    mixed_ref, o_ref,
    wg, wu, wd, wo, out, arr, part, half_in, quart_in, ret, c_hi, c_lo,
    kv, m_ref, l_ref, acc_ref, heads_ref,
    w_sem, a2a_send, a2a_recv, ag_send, ag_recv, fw_send, fw_recv,
    hs_send, hs_recv, qa_send, qa_recv, qb_send, qb_recv, ret_send, ret_recv,
    kz_send, kz_recv, ky_send, ky_recv, kf_send, kf_recv, ks_send, ks_recv,
):
    e = lax.axis_index("ep")
    x = lax.axis_index("tp")
    n_ep = nz * nk
    ny = nk // 2
    z, k_own = e // nk, e % nk
    y, core = k_own // 2, k_own % 2
    right, left, far = (x + 1) % nx, (x + nx - 1) % nx, (x + 2) % nx
    rows, width = tok_ref.shape
    quarter = width // nx
    chunk_rows = nk * CAP
    half = chunk_rows // 2
    q_rows = q_ref.shape[0]
    heads = q_ref.shape[1] // HD
    block_rows = kv.shape[2]

    barrier = pltpu.get_barrier_semaphore()

    @pl.loop(1, n_ep)
    def _(k):
        pl.semaphore_signal(barrier, inc=1, device_id=((e + k) % n_ep, x), device_id_type=MESH)

    for side in (left, right):
        pl.semaphore_signal(barrier, inc=1, device_id=(e, side), device_id_type=MESH)

    own_kv = [
        pltpu.make_async_copy(key_hbm, kv.at[z, k_own, pl.ds(0, q_rows)], w_sem.at[4]),
        pltpu.make_async_copy(value_hbm, kv.at[z, k_own, pl.ds(q_rows, q_rows)], w_sem.at[5]),
    ]
    loads = [
        pltpu.make_async_copy(src, dst, w_sem.at[i])
        for i, (src, dst) in enumerate(((wg_hbm, wg), (wu_hbm, wu), (wd_hbm, wd), (wo_hbm, wo)))
    ]
    for load in own_kv + loads:
        load.start()

    lines = lines_ref[...]
    g_hi = lines.astype(BF16)
    rest = lines - g_hi.astype(F32)
    g_mid = rest.astype(BF16)
    g_lo = (rest - g_mid.astype(F32)).astype(BF16)
    n_lines = lines.shape[0]
    kv[z, k_own, 2 * q_rows :, :] = jnp.concatenate(
        [g_hi.astype(F32), g_mid.astype(F32), g_lo.astype(F32), jnp.zeros_like(lines)], axis=0
    ).astype(BF16)

    rt = routes_t_ref[...]
    e_row = iota((n_ep, rows), 0)
    named = jnp.zeros((n_ep, rows), F32)
    for k in range(rt.shape[0]):
        named = named + (rt[k : k + 1, :] == e_row).astype(F32)
    before = (iota((rows, rows), 0) < iota((rows, rows), 1)).astype(BF16)
    named = named.astype(BF16)
    rank = dot(named, before).astype(BF16)

    tokens = tok_ref[...].astype(F32)
    inv = lax.rsqrt(jnp.mean(tokens * tokens, axis=-1, keepdims=True) + 1e-06)
    mine = pl.ds(pl.multiple_of(x * quarter, quarter), quarter)
    normed = (tok_ref[:, mine].astype(F32) * inv * gain_ref[:, mine]).astype(BF16)

    @pl.loop(0, nz)
    def _(block):
        base = block * chunk_rows
        slot = iota((chunk_rows, n_ep), 0) + base
        spread = ((slot // CAP) == iota((chunk_rows, n_ep), 1)).astype(BF16)
        hit = (dot(spread, named) > 0.5) & (
            dot(spread, rank) == ((iota((chunk_rows, rows), 0) + base) % CAP).astype(F32)
        )
        at = pl.ds(pl.multiple_of(base, chunk_rows), chunk_rows)
        out[at, :] = dot(hit.astype(BF16), normed).astype(BF16)

    for load in own_kv:
        load.wait()
    pl.semaphore_wait(barrier, n_ep - 1 + 2)

    def dz_of(c):
        return jnp.where(c % 2 == 1, (c + 1) // 2, (nz - c // 2) % nz)

    def slot_rows(index):
        return pl.ds(pl.multiple_of(index * CAP, CAP), CAP)

    def await_bytes(ref, sem):
        pltpu.make_async_copy(ref, ref, sem).wait()

    def send(src, dst, send_sem, recv_sem, to):
        pltpu.make_async_remote_copy(
            src, dst, send_sem, recv_sem, device_id=(e, to), device_id_type=MESH
        ).start()

    def send_block(ref, send_sem, recv_sem, to):
        pltpu.make_async_remote_copy(
            ref, ref, send_sem, recv_sem, device_id=(to, x), device_id_type=MESH
        ).start()

    def dispatch(c):
        dest_z = (z + dz_of(c)) % nz

        @pl.loop(jnp.where(c == 0, 1, 0), nk)
        def _(k):
            dest = dest_z * nk + (k_own + k) % nk
            pltpu.make_async_remote_copy(
                out.at[slot_rows(dest)],
                arr.at[x, c, slot_rows(k_own)],
                a2a_send.at[c],
                a2a_recv.at[c],
                device_id=(dest, x),
                device_id_type=MESH,
            ).start()

    ahead = min(AHEAD, nz)

    @pl.loop(0, ahead)
    def _(c):
        dispatch(c)

    arr[x, 0, slot_rows(k_own), :] = out[slot_rows(e), :]

    routes = routes_ref[...]
    e_col = iota((rows, n_ep), 1)
    named2 = jnp.zeros((rows, n_ep), F32)
    weight = jnp.zeros((rows, n_ep), F32)
    for k in range(routes.shape[1]):
        hit = routes[:, k : k + 1] == e_col
        named2 = named2 + hit.astype(F32)
        weight = weight + jnp.where(hit, rw_ref[:, k : k + 1], 0.0)
    named2 = named2.astype(BF16)
    earlier = (iota((rows, rows), 1) < iota((rows, rows), 0)).astype(BF16)
    rank2 = dot(earlier, named2).astype(BF16)
    w_hi = weight.astype(BF16)
    w_lo = (weight - w_hi.astype(F32)).astype(BF16)

    slot = iota((n_ep, n_ep * CAP), 1)
    spread = ((slot // CAP) == iota((n_ep, n_ep * CAP), 0)).astype(BF16)
    keep = (dot(named2, spread) > 0.5) & (
        dot(rank2, spread) == (iota((rows, n_ep * CAP), 1) % CAP).astype(F32)
    )
    c_hi[...] = jnp.where(keep, dot(w_hi, spread), 0.0).astype(BF16)
    c_lo[...] = jnp.where(keep, dot(w_lo, spread), 0.0).astype(BF16)

    m_ref[...] = jnp.full_like(m_ref, FLOOR)
    l_ref[...] = jnp.zeros_like(l_ref)
    acc_ref[...] = jnp.zeros_like(acc_ref)
    halves = q_rows // 128
    ratio = HD ** (-0.5) * LOG2E

    def visit(zs, p, masked):
        both = pl.ds(2 * p, 2)
        key = kv[zs, both, 0:q_rows, :].reshape(2 * q_rows, HD)
        value = kv[zs, both, q_rows : 2 * q_rows, :].reshape(2 * q_rows, HD)
        terms = kv[zs, both, 2 * q_rows :, :].astype(F32)
        n = n_lines
        gates = terms[:, 0:n] + terms[:, n : 2 * n] + terms[:, 2 * n : 3 * n]
        if masked:
            pos = p * 2 * q_rows + iota((q_rows, 2 * q_rows), 1)
            own_pos = k_own * q_rows + iota((q_rows, 2 * q_rows), 0)
            allowed = pos <= own_pos
        for h in range(heads):
            line = jnp.concatenate(
                [gates[b, h * halves + i : h * halves + i + 1, :] for b in range(2) for i in range(halves)],
                axis=1,
            )
            line = (line - lines_ref[h * halves : h * halves + 1, 0:1]) * LOG2E
            s = lax.dot_general(
                q_ref[:, h * HD : (h + 1) * HD], key, (((1,), (1,)), ((), ())), preferred_element_type=F32
            )
            t = s * ratio - line
            if masked:
                t = jnp.where(allowed, t, FLOOR)
            old = m_ref[h]
            new = jnp.maximum(old, jnp.max(t, axis=1, keepdims=True))
            alpha = jnp.exp2(old - new)
            w = jnp.exp2(t - new)
            l_ref[h] = alpha * l_ref[h] + jnp.sum(w, axis=1, keepdims=True)
            acc_ref[h] = alpha * acc_ref[h] + dot(w.astype(BF16), value)
            m_ref[h] = new

    low, high = pl.ds(0, half), pl.ds(half, half)
    first_rows = pl.ds(0, (nk - 1) * CAP)
    b_low, b_high = pl.ds(0, block_rows // 2), pl.ds(block_rows // 2, block_rows // 2)
    y_up, y_down, y_far = (y + 1) % ny, (y + ny - 1) % ny, (y + 2) % ny
    plane = z * nk
    up_dev, down_dev = plane + y_up * 2 + core, plane + y_down * 2 + core
    sibling = plane + y * 2 + (1 - core)

    def scatter_sends(c):
        send(part.at[far, c, low], half_in.at[0, c], hs_send.at[0, c], hs_recv.at[0, c], right)
        send(part.at[far, c, high], half_in.at[1, c], hs_send.at[1, c], hs_recv.at[1, c], left)
        send(part.at[right, c, high], quart_in.at[0, c, high], qa_send.at[0, c], qa_recv.at[0, c], right)
        send(part.at[left, c, low], quart_in.at[1, c, low], qa_send.at[1, c], qa_recv.at[1, c], left)

    @pl.loop(0, nz + 6)
    def _(step):
        @pl.when((step >= 3) & (step < nz + 5))
        def _():
            c = step - 3
            await_bytes(half_in.at[0, c], hs_recv.at[0, c])
            part[right, c, 0:half, :] = (
                part[right, c, 0:half, :].astype(F32) + half_in[0, c].astype(F32)
            ).astype(BF16)
            send(part.at[right, c, low], quart_in.at[0, c, low], qb_send.at[0, c], qb_recv.at[0, c], right)
            await_bytes(half_in.at[1, c], hs_recv.at[1, c])
            part[left, c, half:, :] = (
                part[left, c, half:, :].astype(F32) + half_in[1, c].astype(F32)
            ).astype(BF16)
            send(part.at[left, c, high], quart_in.at[1, c, high], qb_send.at[1, c], qb_recv.at[1, c], left)

        @pl.when(step >= 4)
        def _():
            c = step - 4
            await_bytes(quart_in.at[0, c, high], qa_recv.at[0, c])
            await_bytes(quart_in.at[1, c, low], qa_recv.at[1, c])
            await_bytes(quart_in.at[0, c, low], qb_recv.at[0, c])
            await_bytes(quart_in.at[1, c, high], qb_recv.at[1, c])
            part[x, c] = (
                part[x, c].astype(F32) + quart_in[0, c].astype(F32) + quart_in[1, c].astype(F32)
            ).astype(BF16)

            @pl.when(c < nz)
            def _():
                home_z = (z + nz - dz_of(c)) % nz

                @pl.loop(jnp.where(c == 0, 1, 0), nk)
                def _(k):
                    k_home = (k_own + k) % nk
                    pltpu.make_async_remote_copy(
                        part.at[x, c, slot_rows(k_home)],
                        ret.at[slot_rows(e)],
                        ret_send.at[c],
                        ret_recv,
                        device_id=(home_z * nk + k_home, x),
                        device_id_type=MESH,
                    ).start()

        @pl.when(step == 2)
        def _():
            for load in loads[:3]:
                load.wait()

        @pl.when((step >= 2) & (step < nz + 2))
        def _():
            c = step - 2
            await_bytes(arr.at[far, c, low], fw_recv.at[0, c])
            await_bytes(arr.at[far, c, high], fw_recv.at[1, c])
            gate = jnp.zeros((chunk_rows, wg.shape[1]), F32)
            up = jnp.zeros((chunk_rows, wg.shape[1]), F32)
            for q in range(nx):
                rows_q = arr[q, c]
                gate = gate + dot(rows_q, wg[q * quarter : (q + 1) * quarter, :])
                up = up + dot(rows_q, wu[q * quarter : (q + 1) * quarter, :])
            hidden = (gate * jax.nn.sigmoid(gate) * up).astype(BF16)
            for q in range(nx):
                part[q, c] = dot(hidden, wd[:, q * quarter : (q + 1) * quarter]).astype(BF16)
            scatter_sends(c)

        @pl.when((step >= 1) & (step < nz + 1))
        def _():
            c = step - 1
            await_bytes(arr.at[left, c], ag_recv.at[0, c])
            send(arr.at[left, c, low], arr.at[left, c, low], fw_send.at[0, c], fw_recv.at[0, c], right)
            await_bytes(arr.at[right, c], ag_recv.at[1, c])
            send(arr.at[right, c, high], arr.at[right, c, high], fw_send.at[1, c], fw_recv.at[1, c], left)

        @pl.when(step < nz)
        def _():
            c = step

            @pl.when(c == 0)
            def _():
                await_bytes(arr.at[x, 0, first_rows], a2a_recv.at[0])

            @pl.when(c > 0)
            def _():
                await_bytes(arr.at[x, c], a2a_recv.at[c])

            send(arr.at[x, c], arr.at[x, c], ag_send.at[0, c], ag_recv.at[0, c], right)
            send(arr.at[x, c], arr.at[x, c], ag_send.at[1, c], ag_recv.at[1, c], left)

        @pl.when((step >= 3) & (step < nz + 3) & (step - 3 <= z))
        def _():
            d = step - 3
            zs = z - d
            for i, line_y in enumerate((y, y_down, y_up, y_far)):
                await_bytes(kv.at[zs, line_y * 2 + 1 - core], ks_recv.at[i, d])

            @pl.loop(0, jnp.where(d == 0, k_own // 2, nk // 2))
            def _(p):
                visit(zs, p, False)

            @pl.when(d == 0)
            def _():
                visit(zs, k_own // 2, True)

        @pl.when((step >= 2) & (step < nz + 2) & (step - 2 <= z))
        def _():
            d = step - 2
            zs = z - d
            opposite = y_far * 2 + core
            await_bytes(kv.at[zs, opposite, b_low], kf_recv.at[0, d])
            await_bytes(kv.at[zs, opposite, b_high], kf_recv.at[1, d])
            send_block(kv.at[zs, opposite], ks_send.at[3, d], ks_recv.at[3, d], sibling)

        @pl.when((step >= 1) & (step < nz + 1) & (step - 1 <= z))
        def _():
            d = step - 1
            zs = z - d
            below = kv.at[zs, y_down * 2 + core]
            await_bytes(below, ky_recv.at[0, d])
            part_low = kv.at[zs, y_down * 2 + core, b_low]
            send_block(part_low, kf_send.at[0, d], kf_recv.at[0, d], up_dev)
            send_block(below, ks_send.at[1, d], ks_recv.at[1, d], sibling)
            above = kv.at[zs, y_up * 2 + core]
            await_bytes(above, ky_recv.at[1, d])
            part_high = kv.at[zs, y_up * 2 + core, b_high]
            send_block(part_high, kf_send.at[1, d], kf_recv.at[1, d], down_dev)
            send_block(above, ks_send.at[2, d], ks_recv.at[2, d], sibling)

        @pl.when((step < nz) & (step <= z))
        def _():
            d = step
            block = kv.at[z - d, k_own]

            @pl.when(d > 0)
            def _():
                await_bytes(block, kz_recv.at[d])

            @pl.when(z + 1 < nz)
            def _():
                send_block(block, kz_send.at[d], kz_recv.at[d + 1], e + nk)

            send_block(block, ky_send.at[0, d], ky_recv.at[0, d], up_dev)
            send_block(block, ky_send.at[1, d], ky_recv.at[1, d], down_dev)
            send_block(block, ks_send.at[0, d], ks_recv.at[0, d], sibling)

        @pl.when(step + ahead < nz)
        def _():
            dispatch(step + ahead)

        @pl.when(step == nz + 2)
        def _():
            loads[3].wait()
            for h in range(heads):
                heads_ref[:, h * HD : (h + 1) * HD] = (acc_ref[h] / l_ref[h]).astype(BF16)
            for n in range(nx):
                mixed = dot(heads_ref[...], wo[:, n * quarter : (n + 1) * quarter]).astype(BF16)
                for q in range(nx):
                    part[q, nz + n // 2, n % 2 * half : n % 2 * half + half, :] = mixed[
                        q * half : (q + 1) * half, :
                    ]
            scatter_sends(nz)
            scatter_sends(nz + 1)

    for n in range(nx):
        mixed_ref[:, n * quarter : (n + 1) * quarter] = part[
            x, nz + n // 2, n % 2 * half : n % 2 * half + half, :
        ]

    ret[slot_rows(e), :] = part[x, 0, slot_rows(k_own), :]
    await_bytes(ret.at[pl.ds(0, (n_ep - 1) * CAP)], ret_recv)
    o_ref[...] = (dot(c_hi[...], ret[...]) + dot(c_lo[...], ret[...])).astype(BF16)

    await_bytes(part.at[x, 0, first_rows], ret_send.at[0])
    await_bytes(arr.at[0, 0, first_rows], a2a_send.at[0])

    @pl.loop(1, nz)
    def _(c):
        await_bytes(part.at[x, c], ret_send.at[c])
        await_bytes(arr.at[0, c], a2a_send.at[c])

    @pl.loop(0, nz)
    def _(c):
        for side in (0, 1):
            await_bytes(arr.at[0, c], ag_send.at[side, c])
            await_bytes(half_in.at[side, c], fw_send.at[side, c])

        @pl.when(c <= z)
        def _():
            block = kv.at[0, 0]

            @pl.when(z + 1 < nz)
            def _():
                await_bytes(block, kz_send.at[c])

            for side in (0, 1):
                await_bytes(block, ky_send.at[side, c])
                await_bytes(kv.at[0, 0, b_low], kf_send.at[side, c])
            for i in range(4):
                await_bytes(block, ks_send.at[i, c])

    @pl.loop(0, nz + 2)
    def _(c):
        for side in (0, 1):
            for sem in (hs_send, qa_send, qb_send):
                await_bytes(half_in.at[side, c], sem.at[side, c])


def per_device(
    queries, keys, values, cum_gates, out_proj,
    tokens, norm_gain, routes, route_weights, w_gate, w_up, w_down,
):
    rows, width = tokens.shape
    q_rows = queries.shape[0]
    heads = cum_gates.shape[1]
    n_ep, nx = lax.axis_size("ep"), lax.axis_size("tp")
    nk = NYC
    nz = n_ep // nk
    quarter = width // nx
    hidden = w_gate.shape[2]
    chunk = nk * CAP
    slots = n_ep * CAP
    lines = cum_gates.T.reshape(heads * q_rows // 128, 128)
    block_rows = 2 * q_rows + 4 * lines.shape[0]
    vmem = pl.BlockSpec(memory_space=pltpu.VMEM)
    anywhere = pl.BlockSpec(memory_space=pl.ANY)
    dma = pltpu.SemaphoreType.DMA
    pair = dma((2, nz))
    more = dma((2, nz + 2))
    line = dma((nz + 1,))
    return pl.pallas_call(
        functools.partial(step_kernel, nz, nk, nx),
        out_shape=(
            jax.ShapeDtypeStruct((q_rows // nx, width), BF16),
            jax.ShapeDtypeStruct((rows, quarter), BF16),
        ),
        in_specs=[vmem] * 7 + [anywhere] * 6,
        out_specs=(vmem, vmem),
        scratch_shapes=[
            pltpu.VMEM((width, hidden), BF16),
            pltpu.VMEM((width, hidden), BF16),
            pltpu.VMEM((hidden, width), BF16),
            pltpu.VMEM(out_proj.shape, BF16),
            pltpu.VMEM((slots, quarter), BF16),
            pltpu.VMEM((nx, nz, chunk, quarter), BF16),
            pltpu.VMEM((nx, nz + 2, chunk, quarter), BF16),
            pltpu.VMEM((2, nz + 2, chunk // 2, quarter), BF16),
            pltpu.VMEM((2, nz + 2, chunk, quarter), BF16),
            pltpu.VMEM((slots, quarter), BF16),
            pltpu.VMEM((rows, slots), BF16),
            pltpu.VMEM((rows, slots), BF16),
            pltpu.VMEM((nz, nk, block_rows, HD), BF16),
            pltpu.VMEM((heads, q_rows, 1), F32),
            pltpu.VMEM((heads, q_rows, 1), F32),
            pltpu.VMEM((heads, q_rows, HD), F32),
            pltpu.VMEM((q_rows, heads * HD), BF16),
            dma((6,)),
            dma((nz,)), dma((nz,)),
            pair, pair, pair, pair,
            more, more, more, more, more, more,
            dma((nz,)),
            dma,
            line, line, pair, pair, pair, pair, dma((4, nz)), dma((4, nz)),
        ],
        compiler_params=pltpu.CompilerParams(
            collective_id=0, has_side_effects=True, vmem_limit_bytes=67043328
        ),
        cost_estimate=pl.CostEstimate(
            flops=100 * 10**9, bytes_accessed=10 * 2**20, transcendentals=0
        ),
    )(
        tokens, norm_gain[None], routes, routes.T, route_weights, queries, lines,
        w_gate[0], w_up[0], w_down[0], out_proj, keys, values,
    )


def solution(mesh):
    placed = (
        P("ep", "tp"), P("ep", "tp"), P("ep", "tp"), P("ep", "tp"), P("tp", None),
        P("ep", None), P(), P("ep", None), P("ep", None),
        P("ep", None, "tp"), P("ep", None, "tp"), P("ep", "tp", None),
    )
    return jax.shard_map(
        per_device,
        mesh=mesh,
        in_specs=placed,
        out_specs=(P(("ep", "tp"), None), P("ep", "tp")),
        check_vma=False,
    )
```

```python
import functools
import math

import jax
import jax.numpy as jnp
from jax import lax
from jax.experimental import pallas as pl
from jax.experimental.pallas import tpu as pltpu
from jax.sharding import PartitionSpec as P

HD = 128
CAP = 16
NYC = 8
LOG2E = math.log2(math.e)
MESH = pl.DeviceIdType.MESH
F32 = jnp.float32
BF16 = jnp.bfloat16
FLOOR = -1e30
AHEAD = 2


def iota(shape, dim):
    return lax.broadcasted_iota(jnp.int32, shape, dim)


def dot(a, b):
    return jnp.dot(a, b, preferred_element_type=F32)


def step_kernel(
    nz, nk, nx,
    tok_ref, gain_ref, routes_ref, rw_ref, q_ref, gates_ref,
    wg_hbm, wu_hbm, wd_hbm, wo_hbm, key_hbm, value_hbm,
    mixed_ref, o_ref,
    wg, wu, wd, wo, out, arr, part, half_in, quart_in, ret, c_hi, c_lo,
    kv, m_ref, l_ref, acc_ref, heads_ref, norm_ref, wide,
    w_sem, a2a_send, a2a_recv, ag_send, ag_recv, fw_send, fw_recv,
    hs_send, hs_recv, qa_send, qa_recv, qb_send, qb_recv, ret_send, ret_recv,
    kz_send, kz_recv, ky_send, ky_recv, kf_send, kf_recv, ks_send, ks_recv,
):
    e = lax.axis_index("ep")
    x = lax.axis_index("tp")
    n_ep = nz * nk
    ny = nk // 2
    z, k_own = e // nk, e % nk
    y, core = k_own // 2, k_own % 2
    right, left, far = (x + 1) % nx, (x + nx - 1) % nx, (x + 2) % nx
    rows, width = tok_ref.shape
    quarter = width // nx
    chunk_rows = nk * CAP
    half = chunk_rows // 2
    q_rows = q_ref.shape[0]
    heads = q_ref.shape[1] // HD
    block_rows = kv.shape[2]

    barrier = pltpu.get_barrier_semaphore()

    @pl.loop(1, n_ep)
    def _(k):
        pl.semaphore_signal(barrier, inc=1, device_id=((e + k) % n_ep, x), device_id_type=MESH)

    for side in (left, right):
        pl.semaphore_signal(barrier, inc=1, device_id=(e, side), device_id_type=MESH)

    own_kv = [
        pltpu.make_async_copy(key_hbm, kv.at[z, k_own, pl.ds(0, q_rows)], w_sem.at[4]),
        pltpu.make_async_copy(value_hbm, kv.at[z, k_own, pl.ds(q_rows, q_rows)], w_sem.at[5]),
    ]
    loads = [
        pltpu.make_async_copy(src, dst, w_sem.at[i])
        for i, (src, dst) in enumerate(((wg_hbm, wg), (wu_hbm, wu), (wd_hbm, wd), (wo_hbm, wo)))
    ]
    for load in own_kv + loads:
        load.start()

    lines = jnp.concatenate(
        [
            gates_ref[h : h + 1, i * 128 : (i + 1) * 128]
            for h in range(heads)
            for i in range(q_rows // 128)
        ],
        axis=0,
    )
    g_hi = lines.astype(BF16)
    rest = lines - g_hi.astype(F32)
    g_mid = rest.astype(BF16)
    g_lo = (rest - g_mid.astype(F32)).astype(BF16)
    n_lines = lines.shape[0]
    kv[z, k_own, 2 * q_rows :, :] = jnp.concatenate(
        [g_hi.astype(F32), g_mid.astype(F32), g_lo.astype(F32), jnp.zeros_like(lines)], axis=0
    ).astype(BF16)

    routes = routes_ref[...]
    e_row = iota((n_ep, rows), 0)
    named = jnp.zeros((n_ep, rows), F32)
    weight = jnp.zeros((n_ep, rows), F32)
    for k in range(routes.shape[0]):
        hit = routes[k : k + 1, :] == e_row
        named = named + hit.astype(F32)
        weight = weight + jnp.where(hit, rw_ref[k : k + 1, :], 0.0)
    before = (iota((rows, rows), 0) < iota((rows, rows), 1)).astype(BF16)
    named = named.astype(BF16)
    rank = dot(named, before).astype(BF16)

    tokens = tok_ref[...].astype(F32)
    inv = lax.rsqrt(jnp.mean(tokens * tokens, axis=-1, keepdims=True) + 1e-06)
    norm_ref[...] = (tokens * inv * gain_ref[...]).astype(BF16)
    normed = norm_ref[:, pl.ds(pl.multiple_of(x * quarter, quarter), quarter)]

    def picks(base):
        slot = iota((chunk_rows, n_ep), 0) + base
        spread = ((slot // CAP) == iota((chunk_rows, n_ep), 1)).astype(BF16)
        hit = (dot(spread, named) > 0.5) & (
            dot(spread, rank) == ((iota((chunk_rows, rows), 0) + base) % CAP).astype(F32)
        )
        return hit.astype(BF16)

    order = [0, nz // 2]
    for near in range(1, (nz + 1) // 2):
        order[-1:-1] = [near, nz - near]
    if nz > 4:
        order[4], order[-1] = order[-1], order[4]

    def dz_of(c):
        return sum(jnp.where(c == i, dz, 0) for i, dz in enumerate(order))

    def prepare(c):
        base = (z + dz_of(c)) % nz * chunk_rows
        at = pl.ds(pl.multiple_of(base, chunk_rows), chunk_rows)
        out[at, :] = dot(picks(base), normed).astype(BF16)

    prepare(1)

    for load in own_kv:
        load.wait()
    pl.semaphore_wait(barrier, n_ep - 1 + 2)

    def slot_rows(index):
        return pl.ds(pl.multiple_of(index * CAP, CAP), CAP)

    def await_bytes(ref, sem):
        pltpu.make_async_copy(ref, ref, sem).wait()

    def send(src, dst, send_sem, recv_sem, to):
        pltpu.make_async_remote_copy(
            src, dst, send_sem, recv_sem, device_id=(e, to), device_id_type=MESH
        ).start()

    def send_block(ref, send_sem, recv_sem, to):
        pltpu.make_async_remote_copy(
            ref, ref, send_sem, recv_sem, device_id=(to, x), device_id_type=MESH
        ).start()

    def dispatch(c):
        dest_z = (z + dz_of(c)) % nz

        @pl.loop(0, nk)
        def _(k):
            dest = dest_z * nk + (k_own + k) % nk
            pltpu.make_async_remote_copy(
                out.at[slot_rows(dest)],
                arr.at[x, c, slot_rows(k_own)],
                a2a_send.at[c],
                a2a_recv.at[c],
                device_id=(dest, x),
                device_id_type=MESH,
            ).start()

    b_low, b_high = pl.ds(0, block_rows // 2), pl.ds(block_rows // 2, block_rows // 2)
    y_up, y_down, y_far = (y + 1) % ny, (y + ny - 1) % ny, (y + 2) % ny
    plane = z * nk
    up_dev, down_dev = plane + y_up * 2 + core, plane + y_down * 2 + core
    sibling = plane + y * 2 + (1 - core)

    def spread_column(d):
        block = kv.at[z - d, k_own]

        @pl.when(z + 1 < nz)
        def _():
            send_block(block, kz_send.at[d], kz_recv.at[d + 1], e + nk)

        send_block(block, ky_send.at[0, d], ky_recv.at[0, d], up_dev)
        send_block(block, ky_send.at[1, d], ky_recv.at[1, d], down_dev)
        send_block(block, ks_send.at[0, d], ks_recv.at[0, d], sibling)

    dispatch(1)
    spread_column(0)

    @pl.loop(2, min(AHEAD, nz - 1) + 1)
    def _(c):
        prepare(c)
        dispatch(c)

    near = picks(z * chunk_rows)
    for q in range(nx):
        wide[q] = dot(near, norm_ref[:, q * quarter : (q + 1) * quarter]).astype(BF16)

    def dispatch_near(q):
        @pl.loop(1, nk)
        def _(k):
            k_dest = (k_own + k) % nk
            pltpu.make_async_remote_copy(
                wide.at[q, slot_rows(k_dest)],
                arr.at[q, 0, slot_rows(k_own)],
                a2a_send.at[0],
                a2a_recv.at[0],
                device_id=(plane + k_dest, x),
                device_id_type=MESH,
            ).start()

    arr[:, 0, slot_rows(k_own), :] = wide[:, slot_rows(k_own), :]

    same = (iota((rows, rows), 0) == iota((rows, rows), 1)).astype(BF16)

    def turned(a):
        return lax.dot_general(
            same, a, (((1,), (1,)), ((), ())), preferred_element_type=F32
        ).astype(BF16)

    w_hi = weight.astype(BF16)
    w_lo = (weight - w_hi.astype(F32)).astype(BF16)
    slot = iota((n_ep, n_ep * CAP), 1)
    spread = ((slot // CAP) == iota((n_ep, n_ep * CAP), 0)).astype(BF16)
    keep = (dot(turned(named), spread) > 0.5) & (
        dot(turned(rank), spread) == (iota((rows, n_ep * CAP), 1) % CAP).astype(F32)
    )
    c_hi[...] = jnp.where(keep, dot(turned(w_hi), spread), 0.0).astype(BF16)
    c_lo[...] = jnp.where(keep, dot(turned(w_lo), spread), 0.0).astype(BF16)

    m_ref[...] = jnp.full_like(m_ref, FLOOR)
    l_ref[...] = jnp.zeros_like(l_ref)
    acc_ref[...] = jnp.zeros_like(acc_ref)
    halves = q_rows // 128
    ratio = HD ** (-0.5) * LOG2E

    def visit(zs, p, masked):
        both = pl.ds(2 * p, 2)
        key = kv[zs, both, 0:q_rows, :].reshape(2 * q_rows, HD)
        value = kv[zs, both, q_rows : 2 * q_rows, :].reshape(2 * q_rows, HD)
        terms = kv[zs, both, 2 * q_rows :, :].astype(F32)
        n = n_lines
        gates = terms[:, 0:n] + terms[:, n : 2 * n] + terms[:, 2 * n : 3 * n]
        if masked:
            pos = p * 2 * q_rows + iota((q_rows, 2 * q_rows), 1)
            own_pos = k_own * q_rows + iota((q_rows, 2 * q_rows), 0)
            allowed = pos <= own_pos
        for h in range(heads):
            line = jnp.concatenate(
                [gates[b, h * halves + i : h * halves + i + 1, :] for b in range(2) for i in range(halves)],
                axis=1,
            )
            line = (line - gates_ref[h : h + 1, 0:1]) * LOG2E
            s = lax.dot_general(
                q_ref[:, h * HD : (h + 1) * HD], key, (((1,), (1,)), ((), ())), preferred_element_type=F32
            )
            t = s * ratio - line
            if masked:
                t = jnp.where(allowed, t, FLOOR)
            old = m_ref[h]
            new = jnp.maximum(old, jnp.max(t, axis=1, keepdims=True))
            alpha = jnp.exp2(old - new)
            w = jnp.exp2(t - new)
            l_ref[h] = alpha * l_ref[h] + jnp.sum(w, axis=1, keepdims=True)
            acc_ref[h] = alpha * acc_ref[h] + dot(w.astype(BF16), value)
            m_ref[h] = new

    low, high = pl.ds(0, half), pl.ds(half, half)
    first_rows = pl.ds(0, (nk - 1) * CAP)
    def half_sends(c):
        send(part.at[far, c, low], half_in.at[0, c], hs_send.at[0, c], hs_recv.at[0, c], right)
        send(part.at[far, c, high], half_in.at[1, c], hs_send.at[1, c], hs_recv.at[1, c], left)

    def quarter_sends(c):
        send(part.at[right, c, high], quart_in.at[0, c, high], qa_send.at[0, c], qa_recv.at[0, c], right)
        send(part.at[left, c, low], quart_in.at[1, c, low], qa_send.at[1, c], qa_recv.at[1, c], left)

    def pass_sums(c):
        await_bytes(half_in.at[0, c], hs_recv.at[0, c])
        part[right, c, 0:half, :] = (
            part[right, c, 0:half, :].astype(F32) + half_in[0, c].astype(F32)
        ).astype(BF16)
        send(part.at[right, c, low], quart_in.at[0, c, low], qb_send.at[0, c], qb_recv.at[0, c], right)
        await_bytes(half_in.at[1, c], hs_recv.at[1, c])
        part[left, c, half:, :] = (
            part[left, c, half:, :].astype(F32) + half_in[1, c].astype(F32)
        ).astype(BF16)
        send(part.at[left, c, high], quart_in.at[1, c, high], qb_send.at[1, c], qb_recv.at[1, c], left)

    def finish(c):
        await_bytes(quart_in.at[0, c, high], qa_recv.at[0, c])
        await_bytes(quart_in.at[1, c, low], qa_recv.at[1, c])
        await_bytes(quart_in.at[0, c, low], qb_recv.at[0, c])
        await_bytes(quart_in.at[1, c, high], qb_recv.at[1, c])
        part[x, c] = (
            part[x, c].astype(F32) + quart_in[0, c].astype(F32) + quart_in[1, c].astype(F32)
        ).astype(BF16)

        @pl.when(c < nz)
        def _():
            home_z = (z + nz - dz_of(c)) % nz

            @pl.loop(jnp.where(c == 0, 1, 0), nk)
            def _(k):
                k_home = (k_own + k) % nk
                pltpu.make_async_remote_copy(
                    part.at[x, c, slot_rows(k_home)],
                    ret.at[slot_rows(e)],
                    ret_send.at[c],
                    ret_recv,
                    device_id=(home_z * nk + k_home, x),
                    device_id_type=MESH,
                ).start()

    def multiply(c):
        gate = jnp.zeros((chunk_rows, wg.shape[1]), F32)
        up = jnp.zeros((chunk_rows, wg.shape[1]), F32)
        for q in range(nx):
            rows_q = arr[q, c]
            gate = gate + dot(rows_q, wg[q * quarter : (q + 1) * quarter, :])
            up = up + dot(rows_q, wu[q * quarter : (q + 1) * quarter, :])
        hidden = (gate * jax.nn.sigmoid(gate) * up).astype(BF16)
        for q in range(nx):
            part[q, c] = dot(hidden, wd[:, q * quarter : (q + 1) * quarter]).astype(BF16)
        half_sends(c)
        quarter_sends(c)

    near_step = nz // 2 + 1
    each = max(1, 2 * nx // nz)

    def planes(turn):
        first = jnp.where(turn <= nz // 2, turn - 1, 2 * turn - nz // 2 - 2)
        return first, jnp.minimum(jnp.where(turn <= nz // 2, turn, first + 2), z + 1)

    last_turn = nz // 2 + nz // 4

    @pl.loop(0, nz + 1)
    def _(step):
        @pl.when(step >= 3)
        def _():
            pass_sums(step - 2)


        @pl.when(step >= 4)
        def _():
            finish(step - 3)


        @pl.when(step >= 2)
        def _():
            c = step - 1

            @pl.when(c == 1)
            def _():
                for load in loads[:3]:
                    load.wait()

            await_bytes(arr.at[far, c, low], fw_recv.at[0, c])
            await_bytes(arr.at[far, c, high], fw_recv.at[1, c])
            multiply(c)

        @pl.when((step >= 1) & (step < nz))
        def _():
            c = step
            await_bytes(arr.at[left, c], ag_recv.at[0, c])
            send(arr.at[left, c, low], arr.at[left, c, low], fw_send.at[0, c], fw_recv.at[0, c], right)
            await_bytes(arr.at[right, c], ag_recv.at[1, c])
            send(arr.at[right, c, high], arr.at[right, c, high], fw_send.at[1, c], fw_recv.at[1, c], left)

        @pl.when(step < nz - 1)
        def _():
            c = step + 1
            await_bytes(arr.at[x, c], a2a_recv.at[c])
            send(arr.at[x, c], arr.at[x, c], ag_send.at[0, c], ag_recv.at[0, c], right)
            send(arr.at[x, c], arr.at[x, c], ag_send.at[1, c], ag_recv.at[1, c], left)

        @pl.when(step == near_step)
        def _():
            await_bytes(arr.at[:, 0, first_rows], a2a_recv.at[0])
            multiply(0)

        @pl.when((step >= 2) & (step <= last_turn + 1))
        def _():
            @pl.loop(*planes(step - 1))
            def _(d):
                zs = z - d
                opposite = y_far * 2 + core
                await_bytes(kv.at[zs, opposite, b_low], kf_recv.at[0, d])
                await_bytes(kv.at[zs, opposite, b_high], kf_recv.at[1, d])
                send_block(kv.at[zs, opposite], ks_send.at[3, d], ks_recv.at[3, d], sibling)

        @pl.when((step >= 1) & (step <= last_turn))
        def _():
            @pl.loop(step, jnp.minimum(jnp.where(step == last_turn, nz, step + 1), z + 1))
            def _(d):
                await_bytes(kv.at[z - d, k_own], kz_recv.at[d])
                spread_column(d)

        @pl.when((step >= 1) & (step <= last_turn))
        def _():
            @pl.loop(*planes(step))
            def _(d):
                zs = z - d
                below = kv.at[zs, y_down * 2 + core]
                await_bytes(below, ky_recv.at[0, d])
                part_low = kv.at[zs, y_down * 2 + core, b_low]
                send_block(part_low, kf_send.at[0, d], kf_recv.at[0, d], up_dev)
                send_block(below, ks_send.at[1, d], ks_recv.at[1, d], sibling)
                above = kv.at[zs, y_up * 2 + core]
                await_bytes(above, ky_recv.at[1, d])
                part_high = kv.at[zs, y_up * 2 + core, b_high]
                send_block(part_high, kf_send.at[1, d], kf_recv.at[1, d], down_dev)
                send_block(above, ks_send.at[2, d], ks_recv.at[2, d], sibling)

        @pl.when(step + AHEAD + 1 < nz)
        def _():
            prepare(step + AHEAD + 1)
            dispatch(step + AHEAD + 1)

        @pl.when((step >= 1) & (step <= nx // each))
        def _():
            @pl.loop((step - 1) * each, step * each)
            def _(q):
                dispatch_near(q)

        @pl.when(step == near_step + 1)
        def _():
            pass_sums(0)

        @pl.when(step == near_step + 2)
        def _():
            finish(0)

        @pl.when((step >= 2) & (step <= last_turn + 1))
        def _():
            @pl.loop(*planes(step - 1))
            def _(d):
                zs = z - d
                for i, line_y in enumerate((y, y_down, y_up, y_far)):
                    await_bytes(kv.at[zs, line_y * 2 + 1 - core], ks_recv.at[i, d])

                @pl.loop(0, jnp.where(d == 0, k_own // 2, nk // 2))
                def _(p):
                    visit(zs, p, False)

                @pl.when(d == 0)
                def _():
                    visit(zs, k_own // 2, True)

    loads[3].wait()
    for h in range(heads):
        heads_ref[:, h * HD : (h + 1) * HD] = (acc_ref[h] / l_ref[h]).astype(BF16)
    for n in range(nx):
        mixed = dot(heads_ref[...], wo[:, n * quarter : (n + 1) * quarter]).astype(BF16)
        for q in range(nx):
            part[q, nz + n // 2, n % 2 * half : n % 2 * half + half, :] = mixed[
                q * half : (q + 1) * half, :
            ]
    if near_step + 2 > nz:
        finish(0)
    finish(nz - 2)
    pass_sums(nz - 1)
    half_sends(nz)
    half_sends(nz + 1)
    quarter_sends(nz)
    quarter_sends(nz + 1)
    finish(nz - 1)

    @pl.loop(nz, nz + 2)
    def _(c):
        pass_sums(c)

    @pl.loop(nz, nz + 2)
    def _(c):
        finish(c)

    for n in range(nx):
        mixed_ref[:, n * quarter : (n + 1) * quarter] = part[
            x, nz + n // 2, n % 2 * half : n % 2 * half + half, :
        ]

    ret[slot_rows(e), :] = part[x, 0, slot_rows(k_own), :]
    await_bytes(ret.at[pl.ds(0, (n_ep - 1) * CAP)], ret_recv)
    o_ref[...] = (dot(c_hi[...], ret[...]) + dot(c_lo[...], ret[...])).astype(BF16)

    await_bytes(part.at[x, 0, first_rows], ret_send.at[0])
    await_bytes(arr.at[:, 0, first_rows], a2a_send.at[0])

    @pl.loop(1, nz)
    def _(c):
        await_bytes(part.at[x, c], ret_send.at[c])
        await_bytes(arr.at[0, c], a2a_send.at[c])

    @pl.loop(0, nz)
    def _(c):
        @pl.when(c > 0)
        def _():
            for side in (0, 1):
                await_bytes(arr.at[0, c], ag_send.at[side, c])
                await_bytes(half_in.at[side, c], fw_send.at[side, c])

        @pl.when(c <= z)
        def _():
            block = kv.at[0, 0]

            @pl.when(z + 1 < nz)
            def _():
                await_bytes(block, kz_send.at[c])

            for side in (0, 1):
                await_bytes(block, ky_send.at[side, c])
                await_bytes(kv.at[0, 0, b_low], kf_send.at[side, c])
            for i in range(4):
                await_bytes(block, ks_send.at[i, c])

    @pl.loop(0, nz + 2)
    def _(c):
        for side in (0, 1):
            for sem in (hs_send, qa_send, qb_send):
                await_bytes(half_in.at[side, c], sem.at[side, c])


def per_device(
    queries, keys, values, cum_gates, out_proj,
    tokens, norm_gain, routes, route_weights, w_gate, w_up, w_down,
):
    rows, width = tokens.shape
    q_rows = queries.shape[0]
    heads = cum_gates.shape[1]
    n_ep, nx = lax.axis_size("ep"), lax.axis_size("tp")
    nk = NYC
    nz = n_ep // nk
    quarter = width // nx
    hidden = w_gate.shape[2]
    chunk = nk * CAP
    slots = n_ep * CAP
    block_rows = 2 * q_rows + 4 * (heads * q_rows // 128)
    vmem = pl.BlockSpec(memory_space=pltpu.VMEM)
    anywhere = pl.BlockSpec(memory_space=pl.ANY)
    dma = pltpu.SemaphoreType.DMA
    pair = dma((2, nz))
    more = dma((2, nz + 2))
    line = dma((nz + 1,))
    return pl.pallas_call(
        functools.partial(step_kernel, nz, nk, nx),
        out_shape=(
            jax.ShapeDtypeStruct((q_rows // nx, width), BF16),
            jax.ShapeDtypeStruct((rows, quarter), BF16),
        ),
        in_specs=[vmem] * 6 + [anywhere] * 6,
        out_specs=(vmem, vmem),
        scratch_shapes=[
            pltpu.VMEM((width, hidden), BF16),
            pltpu.VMEM((width, hidden), BF16),
            pltpu.VMEM((hidden, width), BF16),
            pltpu.VMEM(out_proj.shape, BF16),
            pltpu.VMEM((slots, quarter), BF16),
            pltpu.VMEM((nx, nz, chunk, quarter), BF16),
            pltpu.VMEM((nx, nz + 2, chunk, quarter), BF16),
            pltpu.VMEM((2, nz + 2, chunk // 2, quarter), BF16),
            pltpu.VMEM((2, nz + 2, chunk, quarter), BF16),
            pltpu.VMEM((slots, quarter), BF16),
            pltpu.VMEM((rows, slots), BF16),
            pltpu.VMEM((rows, slots), BF16),
            pltpu.VMEM((nz, nk, block_rows, HD), BF16),
            pltpu.VMEM((heads, q_rows, 1), F32),
            pltpu.VMEM((heads, q_rows, 1), F32),
            pltpu.VMEM((heads, q_rows, HD), F32),
            pltpu.VMEM((q_rows, heads * HD), BF16),
            pltpu.VMEM((rows, width), BF16),
            pltpu.VMEM((nx, chunk, quarter), BF16),
            dma((6,)),
            dma((nz,)), dma((nz,)),
            pair, pair, pair, pair,
            more, more, more, more, more, more,
            dma((nz,)),
            dma,
            line, line, pair, pair, pair, pair, dma((4, nz)), dma((4, nz)),
        ],
        compiler_params=pltpu.CompilerParams(
            collective_id=0, has_side_effects=True, vmem_limit_bytes=67043328
        ),
        cost_estimate=pl.CostEstimate(
            flops=100 * 10**9, bytes_accessed=10 * 2**20, transcendentals=0
        ),
    )(
        tokens, norm_gain[None], routes.T, route_weights.T, queries, cum_gates.T,
        w_gate[0], w_up[0], w_down[0], out_proj, keys, values,
    )


def solution(mesh):
    placed = (
        P("ep", "tp"), P("ep", "tp"), P("ep", "tp"), P("ep", "tp"), P("tp", None),
        P("ep", None), P(), P("ep", None), P("ep", None),
        P("ep", None, "tp"), P("ep", None, "tp"), P("ep", "tp", None),
    )
    return jax.shard_map(
        per_device,
        mesh=mesh,
        in_specs=placed,
        out_specs=(P(("ep", "tp"), None), P("ep", "tp")),
        check_vma=False,
    )
```

```python
import functools
import math

import jax
import jax.numpy as jnp
from jax import lax
from jax.experimental import pallas as pl
from jax.experimental.pallas import tpu as pltpu
from jax.sharding import PartitionSpec as P

HD = 128
CAP = 16
NYC = 8
LOG2E = math.log2(math.e)
MESH = pl.DeviceIdType.MESH
F32 = jnp.float32
BF16 = jnp.bfloat16
FLOOR = -1e30
AHEAD = 3


def iota(shape, dim):
    return lax.broadcasted_iota(jnp.int32, shape, dim)


def dot(a, b):
    return jnp.dot(a, b, preferred_element_type=F32)


def step_kernel(
    nz, nk, nx,
    tok_ref, gain_ref, routes_ref, rw_ref, q_ref, gates_ref,
    wg_hbm, wu_hbm, wd_hbm, wo_hbm, key_hbm, value_hbm,
    mixed_ref, o_ref,
    wg, wu, wd, wo, out, arr, part, half_in, quart_in, ret, c_hi, c_lo,
    kv, m_ref, l_ref, acc_ref, heads_ref, norm_ref, wide,
    w_sem, a2a_send, a2a_recv, ag_send, ag_recv, fw_send, fw_recv,
    hs_send, hs_recv, qa_send, qa_recv, qb_send, qb_recv, ret_send, ret_recv,
    kz_send, kz_recv, ky_send, ky_recv, kf_send, kf_recv, ks_send, ks_recv,
):
    e = lax.axis_index("ep")
    x = lax.axis_index("tp")
    n_ep = nz * nk
    ny = nk // 2
    z, k_own = e // nk, e % nk
    y, core = k_own // 2, k_own % 2
    right, left, far = (x + 1) % nx, (x + nx - 1) % nx, (x + 2) % nx
    rows, width = tok_ref.shape
    quarter = width // nx
    chunk_rows = nk * CAP
    half = chunk_rows // 2
    q_rows = q_ref.shape[0]
    heads = q_ref.shape[1] // HD
    block_rows = kv.shape[2]

    barrier = pltpu.get_barrier_semaphore()

    @pl.loop(1, n_ep)
    def _(k):
        pl.semaphore_signal(barrier, inc=1, device_id=((e + k) % n_ep, x), device_id_type=MESH)

    for side in (left, right):
        pl.semaphore_signal(barrier, inc=1, device_id=(e, side), device_id_type=MESH)

    own_kv = [
        pltpu.make_async_copy(key_hbm, kv.at[z, k_own, pl.ds(0, q_rows)], w_sem.at[4]),
        pltpu.make_async_copy(value_hbm, kv.at[z, k_own, pl.ds(q_rows, q_rows)], w_sem.at[5]),
    ]
    loads = [
        pltpu.make_async_copy(src, dst, w_sem.at[i])
        for i, (src, dst) in enumerate(((wg_hbm, wg), (wu_hbm, wu), (wd_hbm, wd), (wo_hbm, wo)))
    ]
    for load in own_kv + loads:
        load.start()

    lines = jnp.concatenate(
        [
            gates_ref[h : h + 1, i * 128 : (i + 1) * 128]
            for h in range(heads)
            for i in range(q_rows // 128)
        ],
        axis=0,
    )
    g_hi = lines.astype(BF16)
    rest = lines - g_hi.astype(F32)
    g_mid = rest.astype(BF16)
    g_lo = (rest - g_mid.astype(F32)).astype(BF16)
    n_lines = lines.shape[0]
    kv[z, k_own, 2 * q_rows :, :] = jnp.concatenate(
        [g_hi.astype(F32), g_mid.astype(F32), g_lo.astype(F32), jnp.zeros_like(lines)], axis=0
    ).astype(BF16)

    routes = routes_ref[...]
    e_row = iota((n_ep, rows), 0)
    named = jnp.zeros((n_ep, rows), F32)
    weight = jnp.zeros((n_ep, rows), F32)
    for k in range(routes.shape[0]):
        hit = routes[k : k + 1, :] == e_row
        named = named + hit.astype(F32)
        weight = weight + jnp.where(hit, rw_ref[k : k + 1, :], 0.0)
    before = (iota((rows, rows), 0) < iota((rows, rows), 1)).astype(BF16)
    named = named.astype(BF16)
    rank = dot(named, before).astype(BF16)

    tokens = tok_ref[...].astype(F32)
    inv = lax.rsqrt(jnp.mean(tokens * tokens, axis=-1, keepdims=True) + 1e-06)
    norm_ref[...] = (tokens * inv * gain_ref[...]).astype(BF16)
    normed = norm_ref[:, pl.ds(pl.multiple_of(x * quarter, quarter), quarter)]

    def picks(base):
        slot = iota((chunk_rows, n_ep), 0) + base
        spread = ((slot // CAP) == iota((chunk_rows, n_ep), 1)).astype(BF16)
        hit = (dot(spread, named) > 0.5) & (
            dot(spread, rank) == ((iota((chunk_rows, rows), 0) + base) % CAP).astype(F32)
        )
        return hit.astype(BF16)

    middle = [nz // 2]
    for near in range(2, (nz + 1) // 2):
        middle += [nz - near, near]
    order = [0, 1] + middle[1:3] + middle[:1] + middle[3:] + [nz - 1]

    def dz_of(c):
        return sum(jnp.where(c == i, dz, 0) for i, dz in enumerate(order))

    def prepare(c):
        base = (z + dz_of(c)) % nz * chunk_rows
        at = pl.ds(pl.multiple_of(base, chunk_rows), chunk_rows)
        out[at, :] = dot(picks(base), normed).astype(BF16)

    prepare(1)

    for load in own_kv:
        load.wait()
    pl.semaphore_wait(barrier, n_ep - 1 + 2)

    def slot_rows(index):
        return pl.ds(pl.multiple_of(index * CAP, CAP), CAP)

    def await_bytes(ref, sem):
        pltpu.make_async_copy(ref, ref, sem).wait()

    def send(src, dst, send_sem, recv_sem, to):
        pltpu.make_async_remote_copy(
            src, dst, send_sem, recv_sem, device_id=(e, to), device_id_type=MESH
        ).start()

    def send_block(ref, send_sem, recv_sem, to):
        pltpu.make_async_remote_copy(
            ref, ref, send_sem, recv_sem, device_id=(to, x), device_id_type=MESH
        ).start()

    def dispatch(c):
        dest_z = (z + dz_of(c)) % nz

        @pl.loop(0, nk)
        def _(k):
            dest = dest_z * nk + (k_own + k) % nk
            pltpu.make_async_remote_copy(
                out.at[slot_rows(dest)],
                arr.at[x, c, slot_rows(k_own)],
                a2a_send.at[c],
                a2a_recv.at[c],
                device_id=(dest, x),
                device_id_type=MESH,
            ).start()

    b_low, b_high = pl.ds(0, block_rows // 2), pl.ds(block_rows // 2, block_rows // 2)
    y_up, y_down, y_far = (y + 1) % ny, (y + ny - 1) % ny, (y + 2) % ny
    plane = z * nk
    up_dev, down_dev = plane + y_up * 2 + core, plane + y_down * 2 + core
    sibling = plane + y * 2 + (1 - core)

    def spread_column(d):
        block = kv.at[z - d, k_own]

        @pl.when(z + 1 < nz)
        def _():
            send_block(block, kz_send.at[d], kz_recv.at[d + 1], e + nk)

        send_block(block, ky_send.at[0, d], ky_recv.at[0, d], up_dev)
        send_block(block, ky_send.at[1, d], ky_recv.at[1, d], down_dev)
        send_block(block, ks_send.at[0, d], ks_recv.at[0, d], sibling)

    dispatch(1)
    spread_column(0)

    @pl.loop(2, min(AHEAD, nz - 2) + 1)
    def _(c):
        prepare(c)
        dispatch(c)

    below_z = (z + nz - 1) % nz
    for i, to_z in enumerate((z, below_z)):
        near = picks(to_z * chunk_rows)
        for q in range(nx):
            wide[i, q] = dot(near, norm_ref[:, q * quarter : (q + 1) * quarter]).astype(BF16)

    def dispatch_wide(i, q, c, to_z):
        @pl.loop(1 - i, nk)
        def _(k):
            k_dest = (k_own + k) % nk
            pltpu.make_async_remote_copy(
                wide.at[i, q, slot_rows(k_dest)],
                arr.at[q, c, slot_rows(k_own)],
                a2a_send.at[c],
                a2a_recv.at[c],
                device_id=(to_z * nk + k_dest, x),
                device_id_type=MESH,
            ).start()

    arr[:, 0, slot_rows(k_own), :] = wide[0, :, slot_rows(k_own), :]

    same = (iota((rows, rows), 0) == iota((rows, rows), 1)).astype(BF16)

    def turned(a):
        return lax.dot_general(
            same, a, (((1,), (1,)), ((), ())), preferred_element_type=F32
        ).astype(BF16)

    w_hi = weight.astype(BF16)
    w_lo = (weight - w_hi.astype(F32)).astype(BF16)
    slot = iota((n_ep, n_ep * CAP), 1)
    spread = ((slot // CAP) == iota((n_ep, n_ep * CAP), 0)).astype(BF16)
    keep = (dot(turned(named), spread) > 0.5) & (
        dot(turned(rank), spread) == (iota((rows, n_ep * CAP), 1) % CAP).astype(F32)
    )
    c_hi[...] = jnp.where(keep, dot(turned(w_hi), spread), 0.0).astype(BF16)
    c_lo[...] = jnp.where(keep, dot(turned(w_lo), spread), 0.0).astype(BF16)

    m_ref[...] = jnp.full_like(m_ref, FLOOR)
    l_ref[...] = jnp.zeros_like(l_ref)
    acc_ref[...] = jnp.zeros_like(acc_ref)
    halves = q_rows // 128
    ratio = HD ** (-0.5) * LOG2E

    def visit(zs, p, masked):
        both = pl.ds(2 * p, 2)
        key = kv[zs, both, 0:q_rows, :].reshape(2 * q_rows, HD)
        value = kv[zs, both, q_rows : 2 * q_rows, :].reshape(2 * q_rows, HD)
        terms = kv[zs, both, 2 * q_rows :, :].astype(F32)
        n = n_lines
        gates = terms[:, 0:n] + terms[:, n : 2 * n] + terms[:, 2 * n : 3 * n]
        if masked:
            pos = p * 2 * q_rows + iota((q_rows, 2 * q_rows), 1)
            own_pos = k_own * q_rows + iota((q_rows, 2 * q_rows), 0)
            allowed = pos <= own_pos
        for h in range(heads):
            line = jnp.concatenate(
                [gates[b, h * halves + i : h * halves + i + 1, :] for b in range(2) for i in range(halves)],
                axis=1,
            )
            line = (line - gates_ref[h : h + 1, 0:1]) * LOG2E
            s = lax.dot_general(
                q_ref[:, h * HD : (h + 1) * HD], key, (((1,), (1,)), ((), ())), preferred_element_type=F32
            )
            t = s * ratio - line
            if masked:
                t = jnp.where(allowed, t, FLOOR)
            old = m_ref[h]
            new = jnp.maximum(old, jnp.max(t, axis=1, keepdims=True))
            alpha = jnp.exp2(old - new)
            w = jnp.exp2(t - new)
            l_ref[h] = alpha * l_ref[h] + jnp.sum(w, axis=1, keepdims=True)
            acc_ref[h] = alpha * acc_ref[h] + dot(w.astype(BF16), value)
            m_ref[h] = new

    low, high = pl.ds(0, half), pl.ds(half, half)
    first_rows = pl.ds(0, (nk - 1) * CAP)
    def half_sends(c):
        send(part.at[far, c, low], half_in.at[0, c], hs_send.at[0, c], hs_recv.at[0, c], right)
        send(part.at[far, c, high], half_in.at[1, c], hs_send.at[1, c], hs_recv.at[1, c], left)

    def quarter_sends(c):
        send(part.at[right, c, high], quart_in.at[0, c, high], qa_send.at[0, c], qa_recv.at[0, c], right)
        send(part.at[left, c, low], quart_in.at[1, c, low], qa_send.at[1, c], qa_recv.at[1, c], left)

    def pass_sums(c):
        await_bytes(half_in.at[0, c], hs_recv.at[0, c])
        part[right, c, 0:half, :] = (
            part[right, c, 0:half, :].astype(F32) + half_in[0, c].astype(F32)
        ).astype(BF16)
        send(part.at[right, c, low], quart_in.at[0, c, low], qb_send.at[0, c], qb_recv.at[0, c], right)
        await_bytes(half_in.at[1, c], hs_recv.at[1, c])
        part[left, c, half:, :] = (
            part[left, c, half:, :].astype(F32) + half_in[1, c].astype(F32)
        ).astype(BF16)
        send(part.at[left, c, high], quart_in.at[1, c, high], qb_send.at[1, c], qb_recv.at[1, c], left)

    def finish(c):
        await_bytes(quart_in.at[0, c, high], qa_recv.at[0, c])
        await_bytes(quart_in.at[1, c, low], qa_recv.at[1, c])
        await_bytes(quart_in.at[0, c, low], qb_recv.at[0, c])
        await_bytes(quart_in.at[1, c, high], qb_recv.at[1, c])
        part[x, c] = (
            part[x, c].astype(F32) + quart_in[0, c].astype(F32) + quart_in[1, c].astype(F32)
        ).astype(BF16)

        @pl.when(c < nz)
        def _():
            home_z = (z + nz - dz_of(c)) % nz

            @pl.loop(jnp.where(c == 0, 1, 0), nk)
            def _(k):
                k_home = (k_own + k) % nk
                pltpu.make_async_remote_copy(
                    part.at[x, c, slot_rows(k_home)],
                    ret.at[slot_rows(e)],
                    ret_send.at[c],
                    ret_recv,
                    device_id=(home_z * nk + k_home, x),
                    device_id_type=MESH,
                ).start()

    def multiply(c):
        gate = jnp.zeros((chunk_rows, wg.shape[1]), F32)
        up = jnp.zeros((chunk_rows, wg.shape[1]), F32)
        for q in range(nx):
            rows_q = arr[q, c]
            gate = gate + dot(rows_q, wg[q * quarter : (q + 1) * quarter, :])
            up = up + dot(rows_q, wu[q * quarter : (q + 1) * quarter, :])
        hidden = (gate * jax.nn.sigmoid(gate) * up).astype(BF16)
        for q in range(nx):
            part[q, c] = dot(hidden, wd[:, q * quarter : (q + 1) * quarter]).astype(BF16)
        half_sends(c)
        quarter_sends(c)

    near_step = nz // 2 + 1
    each = max(1, 2 * nx // nz)

    def planes(turn):
        first = jnp.where(turn <= nz // 2, turn - 1, 2 * turn - nz // 2 - 2)
        return first, jnp.minimum(jnp.where(turn <= nz // 2, turn, first + 2), z + 1)

    last_turn = nz // 2 + nz // 4

    @pl.loop(0, nz)
    def _(step):
        @pl.when(step >= 3)
        def _():
            pass_sums(step - 2)


        @pl.when(step >= 4)
        def _():
            finish(step - 3)


        @pl.when(step >= 2)
        def _():
            c = step - 1

            @pl.when(c == 1)
            def _():
                for load in loads[:3]:
                    load.wait()

            await_bytes(arr.at[far, c, low], fw_recv.at[0, c])
            await_bytes(arr.at[far, c, high], fw_recv.at[1, c])
            multiply(c)

        @pl.when((step >= 1) & (step < nz - 1))
        def _():
            c = step
            await_bytes(arr.at[left, c], ag_recv.at[0, c])
            send(arr.at[left, c, low], arr.at[left, c, low], fw_send.at[0, c], fw_recv.at[0, c], right)
            await_bytes(arr.at[right, c], ag_recv.at[1, c])
            send(arr.at[right, c, high], arr.at[right, c, high], fw_send.at[1, c], fw_recv.at[1, c], left)

        @pl.when(step < nz - 3)
        def _():
            @pl.loop(jnp.where(step == 0, 1, step + 2), step + 3)
            def _(c):
                await_bytes(arr.at[x, c], a2a_recv.at[c])
                send(arr.at[x, c], arr.at[x, c], ag_send.at[0, c], ag_recv.at[0, c], right)
                send(arr.at[x, c], arr.at[x, c], ag_send.at[1, c], ag_recv.at[1, c], left)

        @pl.when(step == near_step)
        def _():
            await_bytes(arr.at[:, 0, first_rows], a2a_recv.at[0])
            multiply(0)

        @pl.when((step >= 2) & (step <= last_turn + 1))
        def _():
            @pl.loop(*planes(step - 1))
            def _(d):
                zs = z - d
                opposite = y_far * 2 + core
                await_bytes(kv.at[zs, opposite, b_low], kf_recv.at[0, d])
                await_bytes(kv.at[zs, opposite, b_high], kf_recv.at[1, d])
                send_block(kv.at[zs, opposite], ks_send.at[3, d], ks_recv.at[3, d], sibling)

        @pl.when((step >= 1) & (step <= last_turn))
        def _():
            @pl.loop(step, jnp.minimum(jnp.where(step == last_turn, nz, step + 1), z + 1))
            def _(d):
                await_bytes(kv.at[z - d, k_own], kz_recv.at[d])
                spread_column(d)

        @pl.when((step >= 1) & (step <= last_turn))
        def _():
            @pl.loop(*planes(step))
            def _(d):
                zs = z - d
                below = kv.at[zs, y_down * 2 + core]
                await_bytes(below, ky_recv.at[0, d])
                part_low = kv.at[zs, y_down * 2 + core, b_low]
                send_block(part_low, kf_send.at[0, d], kf_recv.at[0, d], up_dev)
                send_block(below, ks_send.at[1, d], ks_recv.at[1, d], sibling)
                above = kv.at[zs, y_up * 2 + core]
                await_bytes(above, ky_recv.at[1, d])
                part_high = kv.at[zs, y_up * 2 + core, b_high]
                send_block(part_high, kf_send.at[1, d], kf_recv.at[1, d], down_dev)
                send_block(above, ks_send.at[2, d], ks_recv.at[2, d], sibling)

        @pl.when(step + AHEAD + 1 < nz - 1)
        def _():
            prepare(step + AHEAD + 1)
            dispatch(step + AHEAD + 1)

        @pl.when((step >= 1) & (step <= nx // each))
        def _():
            @pl.loop((step - 1) * each, step * each)
            def _(q):
                dispatch_wide(0, q, 0, z)

        @pl.when((step >= 2) & (step <= nx // each + 1))
        def _():
            @pl.loop((step - 2) * each, (step - 1) * each)
            def _(q):
                dispatch_wide(1, q, nz - 1, below_z)

        @pl.when(step == near_step + 1)
        def _():
            pass_sums(0)

        @pl.when(step == near_step + 2)
        def _():
            finish(0)

        @pl.when(step == nz - 1)
        def _():
            await_bytes(arr.at[:, nz - 1], a2a_recv.at[nz - 1])
            multiply(nz - 1)

        @pl.when((step >= 2) & (step <= last_turn + 1))
        def _():
            @pl.loop(*planes(step - 1))
            def _(d):
                zs = z - d
                for i, line_y in enumerate((y, y_down, y_up, y_far)):
                    await_bytes(kv.at[zs, line_y * 2 + 1 - core], ks_recv.at[i, d])

                @pl.loop(0, jnp.where(d == 0, k_own // 2, nk // 2))
                def _(p):
                    visit(zs, p, False)

                @pl.when(d == 0)
                def _():
                    visit(zs, k_own // 2, True)

    loads[3].wait()
    for h in range(heads):
        heads_ref[:, h * HD : (h + 1) * HD] = (acc_ref[h] / l_ref[h]).astype(BF16)
    for n in range(nx):
        mixed = dot(heads_ref[...], wo[:, n * quarter : (n + 1) * quarter]).astype(BF16)
        for q in range(nx):
            part[q, nz + n // 2, n % 2 * half : n % 2 * half + half, :] = mixed[
                q * half : (q + 1) * half, :
            ]
    pass_sums(nz - 2)
    finish(nz - 3)
    pass_sums(nz - 1)
    half_sends(nz)
    half_sends(nz + 1)
    quarter_sends(nz)
    quarter_sends(nz + 1)
    finish(nz - 2)
    finish(nz - 1)

    @pl.loop(nz, nz + 2)
    def _(c):
        pass_sums(c)

    @pl.loop(nz, nz + 2)
    def _(c):
        finish(c)

    for n in range(nx):
        mixed_ref[:, n * quarter : (n + 1) * quarter] = part[
            x, nz + n // 2, n % 2 * half : n % 2 * half + half, :
        ]

    ret[slot_rows(e), :] = part[x, 0, slot_rows(k_own), :]
    await_bytes(ret.at[pl.ds(0, (n_ep - 1) * CAP)], ret_recv)
    o_ref[...] = (dot(c_hi[...], ret[...]) + dot(c_lo[...], ret[...])).astype(BF16)

    await_bytes(part.at[x, 0, first_rows], ret_send.at[0])
    await_bytes(part.at[x, nz - 1], ret_send.at[nz - 1])
    await_bytes(arr.at[:, nz - 1], a2a_send.at[nz - 1])
    await_bytes(arr.at[:, 0, first_rows], a2a_send.at[0])

    @pl.loop(1, nz - 1)
    def _(c):
        await_bytes(part.at[x, c], ret_send.at[c])
        await_bytes(arr.at[0, c], a2a_send.at[c])

    @pl.loop(0, nz)
    def _(c):
        @pl.when((c > 0) & (c < nz - 1))
        def _():
            for side in (0, 1):
                await_bytes(arr.at[0, c], ag_send.at[side, c])
                await_bytes(half_in.at[side, c], fw_send.at[side, c])

        @pl.when(c <= z)
        def _():
            block = kv.at[0, 0]

            @pl.when(z + 1 < nz)
            def _():
                await_bytes(block, kz_send.at[c])

            for side in (0, 1):
                await_bytes(block, ky_send.at[side, c])
                await_bytes(kv.at[0, 0, b_low], kf_send.at[side, c])
            for i in range(4):
                await_bytes(block, ks_send.at[i, c])

    @pl.loop(0, nz + 2)
    def _(c):
        for side in (0, 1):
            for sem in (hs_send, qa_send, qb_send):
                await_bytes(half_in.at[side, c], sem.at[side, c])


def per_device(
    queries, keys, values, cum_gates, out_proj,
    tokens, norm_gain, routes, route_weights, w_gate, w_up, w_down,
):
    rows, width = tokens.shape
    q_rows = queries.shape[0]
    heads = cum_gates.shape[1]
    n_ep, nx = lax.axis_size("ep"), lax.axis_size("tp")
    nk = NYC
    nz = n_ep // nk
    quarter = width // nx
    hidden = w_gate.shape[2]
    chunk = nk * CAP
    slots = n_ep * CAP
    block_rows = 2 * q_rows + 4 * (heads * q_rows // 128)
    vmem = pl.BlockSpec(memory_space=pltpu.VMEM)
    anywhere = pl.BlockSpec(memory_space=pl.ANY)
    dma = pltpu.SemaphoreType.DMA
    pair = dma((2, nz))
    more = dma((2, nz + 2))
    line = dma((nz + 1,))
    return pl.pallas_call(
        functools.partial(step_kernel, nz, nk, nx),
        out_shape=(
            jax.ShapeDtypeStruct((q_rows // nx, width), BF16),
            jax.ShapeDtypeStruct((rows, quarter), BF16),
        ),
        in_specs=[vmem] * 6 + [anywhere] * 6,
        out_specs=(vmem, vmem),
        scratch_shapes=[
            pltpu.VMEM((width, hidden), BF16),
            pltpu.VMEM((width, hidden), BF16),
            pltpu.VMEM((hidden, width), BF16),
            pltpu.VMEM(out_proj.shape, BF16),
            pltpu.VMEM((slots, quarter), BF16),
            pltpu.VMEM((nx, nz, chunk, quarter), BF16),
            pltpu.VMEM((nx, nz + 2, chunk, quarter), BF16),
            pltpu.VMEM((2, nz + 2, chunk // 2, quarter), BF16),
            pltpu.VMEM((2, nz + 2, chunk, quarter), BF16),
            pltpu.VMEM((slots, quarter), BF16),
            pltpu.VMEM((rows, slots), BF16),
            pltpu.VMEM((rows, slots), BF16),
            pltpu.VMEM((nz, nk, block_rows, HD), BF16),
            pltpu.VMEM((heads, q_rows, 1), F32),
            pltpu.VMEM((heads, q_rows, 1), F32),
            pltpu.VMEM((heads, q_rows, HD), F32),
            pltpu.VMEM((q_rows, heads * HD), BF16),
            pltpu.VMEM((rows, width), BF16),
            pltpu.VMEM((2, nx, chunk, quarter), BF16),
            dma((6,)),
            dma((nz,)), dma((nz,)),
            pair, pair, pair, pair,
            more, more, more, more, more, more,
            dma((nz,)),
            dma,
            line, line, pair, pair, pair, pair, dma((4, nz)), dma((4, nz)),
        ],
        compiler_params=pltpu.CompilerParams(
            collective_id=0, has_side_effects=True, vmem_limit_bytes=67043328
        ),
        cost_estimate=pl.CostEstimate(
            flops=100 * 10**9, bytes_accessed=10 * 2**20, transcendentals=0
        ),
    )(
        tokens, norm_gain[None], routes.T, route_weights.T, queries, cum_gates.T,
        w_gate[0], w_up[0], w_down[0], out_proj, keys, values,
    )


def solution(mesh):
    placed = (
        P("ep", "tp"), P("ep", "tp"), P("ep", "tp"), P("ep", "tp"), P("tp", None),
        P("ep", None), P(), P("ep", None), P("ep", None),
        P("ep", None, "tp"), P("ep", None, "tp"), P("ep", "tp", None),
    )
    return jax.shard_map(
        per_device,
        mesh=mesh,
        in_specs=placed,
        out_specs=(P(("ep", "tp"), None), P("ep", "tp")),
        check_vma=False,
    )
```

```python
import functools
import math

import jax
import jax.numpy as jnp
from jax import lax
from jax.experimental import pallas as pl
from jax.experimental.pallas import tpu as pltpu
from jax.sharding import PartitionSpec as P

HD = 128
CAP = 16
NYC = 8
LOG2E = math.log2(math.e)
MESH = pl.DeviceIdType.MESH
F32 = jnp.float32
BF16 = jnp.bfloat16
FLOOR = -1e30
AHEAD = 3


def iota(shape, dim):
    return lax.broadcasted_iota(jnp.int32, shape, dim)


def dot(a, b):
    return jnp.dot(a, b, preferred_element_type=F32)


def step_kernel(
    nz, nk, nx,
    tok_ref, gain_ref, routes_ref, rw_ref, q_ref, gates_ref,
    wg_hbm, wu_hbm, wd_hbm, wo_hbm, key_hbm, value_hbm,
    mixed_ref, o_ref,
    wg, wu, wd, wo, out, arr, part, half_in, quart_in, ret, c_hi, c_lo,
    kv, m_ref, l_ref, acc_ref, heads_ref, norm_ref, wide,
    w_sem, a2a_send, a2a_recv, ag_send, ag_recv, fw_send, fw_recv,
    hs_send, hs_recv, qa_send, qa_recv, qb_send, qb_recv, ret_send, ret_recv,
    kz_send, kz_recv, ky_send, ky_recv, kf_send, kf_recv, ks_send, ks_recv,
):
    e = lax.axis_index("ep")
    x = lax.axis_index("tp")
    n_ep = nz * nk
    ny = nk // 2
    z, k_own = e // nk, e % nk
    y, core = k_own // 2, k_own % 2
    right, left, far = (x + 1) % nx, (x + nx - 1) % nx, (x + 2) % nx
    rows, width = tok_ref.shape
    quarter = width // nx
    chunk_rows = nk * CAP
    half = chunk_rows // 2
    q_rows = q_ref.shape[0]
    heads = q_ref.shape[1] // HD
    block_rows = kv.shape[2]

    barrier = pltpu.get_barrier_semaphore()

    @pl.loop(1, n_ep)
    def _(k):
        pl.semaphore_signal(barrier, inc=1, device_id=((e + k) % n_ep, x), device_id_type=MESH)

    for side in (left, right):
        pl.semaphore_signal(barrier, inc=1, device_id=(e, side), device_id_type=MESH)

    own_kv = [
        pltpu.make_async_copy(key_hbm, kv.at[z, k_own, pl.ds(0, q_rows)], w_sem.at[4]),
        pltpu.make_async_copy(value_hbm, kv.at[z, k_own, pl.ds(q_rows, q_rows)], w_sem.at[5]),
    ]
    loads = [
        pltpu.make_async_copy(src, dst, w_sem.at[i])
        for i, (src, dst) in enumerate(((wg_hbm, wg), (wu_hbm, wu), (wd_hbm, wd), (wo_hbm, wo)))
    ]
    for load in own_kv + loads:
        load.start()

    lines = jnp.concatenate(
        [
            gates_ref[h : h + 1, i * 128 : (i + 1) * 128]
            for h in range(heads)
            for i in range(q_rows // 128)
        ],
        axis=0,
    )
    g_hi = lines.astype(BF16)
    rest = lines - g_hi.astype(F32)
    g_mid = rest.astype(BF16)
    g_lo = (rest - g_mid.astype(F32)).astype(BF16)
    n_lines = lines.shape[0]
    kv[z, k_own, 2 * q_rows :, :] = jnp.concatenate(
        [g_hi.astype(F32), g_mid.astype(F32), g_lo.astype(F32), jnp.zeros_like(lines)], axis=0
    ).astype(BF16)

    routes = routes_ref[...]
    e_row = iota((n_ep, rows), 0)
    named = jnp.zeros((n_ep, rows), F32)
    weight = jnp.zeros((n_ep, rows), F32)
    for k in range(routes.shape[0]):
        hit = routes[k : k + 1, :] == e_row
        named = named + hit.astype(F32)
        weight = weight + jnp.where(hit, rw_ref[k : k + 1, :], 0.0)
    before = (iota((rows, rows), 0) < iota((rows, rows), 1)).astype(BF16)
    named = named.astype(BF16)
    rank = dot(named, before).astype(BF16)

    tokens = tok_ref[...].astype(F32)
    inv = lax.rsqrt(jnp.mean(tokens * tokens, axis=-1, keepdims=True) + 1e-06)
    norm_ref[...] = (tokens * inv * gain_ref[...]).astype(BF16)
    normed = norm_ref[:, pl.ds(pl.multiple_of(x * quarter, quarter), quarter)]

    def picks(base):
        slot = iota((chunk_rows, n_ep), 0) + base
        spread = ((slot // CAP) == iota((chunk_rows, n_ep), 1)).astype(BF16)
        hit = (dot(spread, named) > 0.5) & (
            dot(spread, rank) == ((iota((chunk_rows, rows), 0) + base) % CAP).astype(F32)
        )
        return hit.astype(BF16)

    middle = [nz // 2]
    for near in range(2, (nz + 1) // 2):
        middle += [nz - near, near]
    order = [0, 1] + middle[1:] + middle[:1] + [nz - 1]

    def dz_of(c):
        return sum(jnp.where(c == i, dz, 0) for i, dz in enumerate(order))

    def prepare(c):
        base = (z + dz_of(c)) % nz * chunk_rows
        at = pl.ds(pl.multiple_of(base, chunk_rows), chunk_rows)
        out[at, :] = dot(picks(base), normed).astype(BF16)

    prepare(1)

    for load in own_kv:
        load.wait()
    pl.semaphore_wait(barrier, n_ep - 1 + 2)

    def slot_rows(index):
        return pl.ds(pl.multiple_of(index * CAP, CAP), CAP)

    def await_bytes(ref, sem):
        pltpu.make_async_copy(ref, ref, sem).wait()

    def send(src, dst, send_sem, recv_sem, to):
        pltpu.make_async_remote_copy(
            src, dst, send_sem, recv_sem, device_id=(e, to), device_id_type=MESH
        ).start()

    def send_block(ref, send_sem, recv_sem, to):
        pltpu.make_async_remote_copy(
            ref, ref, send_sem, recv_sem, device_id=(to, x), device_id_type=MESH
        ).start()

    def dispatch(c):
        dest_z = (z + dz_of(c)) % nz

        @pl.loop(0, nk)
        def _(k):
            dest = dest_z * nk + (k_own + k) % nk
            pltpu.make_async_remote_copy(
                out.at[slot_rows(dest)],
                arr.at[x, c, slot_rows(k_own)],
                a2a_send.at[c],
                a2a_recv.at[c],
                device_id=(dest, x),
                device_id_type=MESH,
            ).start()

    b_low, b_high = pl.ds(0, block_rows // 2), pl.ds(block_rows // 2, block_rows // 2)
    y_up, y_down, y_far = (y + 1) % ny, (y + ny - 1) % ny, (y + 2) % ny
    plane = z * nk
    up_dev, down_dev = plane + y_up * 2 + core, plane + y_down * 2 + core
    sibling = plane + y * 2 + (1 - core)

    def spread_column(d):
        block = kv.at[z - d, k_own]

        @pl.when(z + 1 < nz)
        def _():
            send_block(block, kz_send.at[d], kz_recv.at[d + 1], e + nk)

        send_block(block, ky_send.at[0, d], ky_recv.at[0, d], up_dev)
        send_block(block, ky_send.at[1, d], ky_recv.at[1, d], down_dev)
        send_block(block, ks_send.at[0, d], ks_recv.at[0, d], sibling)

    dispatch(1)
    spread_column(0)

    @pl.loop(2, min(AHEAD, nz - 2) + 1)
    def _(c):
        prepare(c)
        dispatch(c)

    below_z = (z + nz - 1) % nz
    for i, to_z in enumerate((z, below_z)):
        near = picks(to_z * chunk_rows)
        for q in range(nx):
            wide[i, q] = dot(near, norm_ref[:, q * quarter : (q + 1) * quarter]).astype(BF16)

    def dispatch_wide(i, q, c, to_z):
        @pl.loop(1 - i, nk)
        def _(k):
            k_dest = (k_own + k) % nk
            pltpu.make_async_remote_copy(
                wide.at[i, q, slot_rows(k_dest)],
                arr.at[q, c, slot_rows(k_own)],
                a2a_send.at[c],
                a2a_recv.at[c],
                device_id=(to_z * nk + k_dest, x),
                device_id_type=MESH,
            ).start()

    arr[:, 0, slot_rows(k_own), :] = wide[0, :, slot_rows(k_own), :]

    same = (iota((rows, rows), 0) == iota((rows, rows), 1)).astype(BF16)

    def turned(a):
        return lax.dot_general(
            same, a, (((1,), (1,)), ((), ())), preferred_element_type=F32
        ).astype(BF16)

    w_hi = weight.astype(BF16)
    w_lo = (weight - w_hi.astype(F32)).astype(BF16)
    slot = iota((n_ep, n_ep * CAP), 1)
    spread = ((slot // CAP) == iota((n_ep, n_ep * CAP), 0)).astype(BF16)
    keep = (dot(turned(named), spread) > 0.5) & (
        dot(turned(rank), spread) == (iota((rows, n_ep * CAP), 1) % CAP).astype(F32)
    )
    c_hi[...] = jnp.where(keep, dot(turned(w_hi), spread), 0.0).astype(BF16)
    c_lo[...] = jnp.where(keep, dot(turned(w_lo), spread), 0.0).astype(BF16)

    m_ref[...] = jnp.full_like(m_ref, FLOOR)
    l_ref[...] = jnp.zeros_like(l_ref)
    acc_ref[...] = jnp.zeros_like(acc_ref)
    halves = q_rows // 128
    ratio = HD ** (-0.5) * LOG2E

    def visit(zs, p, masked):
        both = pl.ds(2 * p, 2)
        key = kv[zs, both, 0:q_rows, :].reshape(2 * q_rows, HD)
        value = kv[zs, both, q_rows : 2 * q_rows, :].reshape(2 * q_rows, HD)
        terms = kv[zs, both, 2 * q_rows :, :].astype(F32)
        n = n_lines
        gates = terms[:, 0:n] + terms[:, n : 2 * n] + terms[:, 2 * n : 3 * n]
        if masked:
            pos = p * 2 * q_rows + iota((q_rows, 2 * q_rows), 1)
            own_pos = k_own * q_rows + iota((q_rows, 2 * q_rows), 0)
            allowed = pos <= own_pos
        for h in range(heads):
            line = jnp.concatenate(
                [gates[b, h * halves + i : h * halves + i + 1, :] for b in range(2) for i in range(halves)],
                axis=1,
            )
            line = (line - gates_ref[h : h + 1, 0:1]) * LOG2E
            s = lax.dot_general(
                q_ref[:, h * HD : (h + 1) * HD], key, (((1,), (1,)), ((), ())), preferred_element_type=F32
            )
            t = s * ratio - line
            if masked:
                t = jnp.where(allowed, t, FLOOR)
            old = m_ref[h]
            new = jnp.maximum(old, jnp.max(t, axis=1, keepdims=True))
            alpha = jnp.exp2(old - new)
            w = jnp.exp2(t - new)
            l_ref[h] = alpha * l_ref[h] + jnp.sum(w, axis=1, keepdims=True)
            acc_ref[h] = alpha * acc_ref[h] + dot(w.astype(BF16), value)
            m_ref[h] = new

    low, high = pl.ds(0, half), pl.ds(half, half)
    first_rows = pl.ds(0, (nk - 1) * CAP)
    def half_sends(c):
        send(part.at[far, c, low], half_in.at[0, c], hs_send.at[0, c], hs_recv.at[0, c], right)
        send(part.at[far, c, high], half_in.at[1, c], hs_send.at[1, c], hs_recv.at[1, c], left)

    def quarter_sends(c):
        send(part.at[right, c, high], quart_in.at[0, c, high], qa_send.at[0, c], qa_recv.at[0, c], right)
        send(part.at[left, c, low], quart_in.at[1, c, low], qa_send.at[1, c], qa_recv.at[1, c], left)

    def pass_sums(c):
        await_bytes(half_in.at[0, c], hs_recv.at[0, c])
        part[right, c, 0:half, :] = (
            part[right, c, 0:half, :].astype(F32) + half_in[0, c].astype(F32)
        ).astype(BF16)
        send(part.at[right, c, low], quart_in.at[0, c, low], qb_send.at[0, c], qb_recv.at[0, c], right)
        await_bytes(half_in.at[1, c], hs_recv.at[1, c])
        part[left, c, half:, :] = (
            part[left, c, half:, :].astype(F32) + half_in[1, c].astype(F32)
        ).astype(BF16)
        send(part.at[left, c, high], quart_in.at[1, c, high], qb_send.at[1, c], qb_recv.at[1, c], left)

    def finish(c):
        await_bytes(quart_in.at[0, c, high], qa_recv.at[0, c])
        await_bytes(quart_in.at[1, c, low], qa_recv.at[1, c])
        await_bytes(quart_in.at[0, c, low], qb_recv.at[0, c])
        await_bytes(quart_in.at[1, c, high], qb_recv.at[1, c])
        part[x, c] = (
            part[x, c].astype(F32) + quart_in[0, c].astype(F32) + quart_in[1, c].astype(F32)
        ).astype(BF16)

        @pl.when(c < nz)
        def _():
            home_z = (z + nz - dz_of(c)) % nz

            @pl.loop(jnp.where(c == 0, 1, 0), nk)
            def _(k):
                k_home = (k_own + k) % nk
                pltpu.make_async_remote_copy(
                    part.at[x, c, slot_rows(k_home)],
                    ret.at[slot_rows(e)],
                    ret_send.at[c],
                    ret_recv,
                    device_id=(home_z * nk + k_home, x),
                    device_id_type=MESH,
                ).start()

    def multiply(c):
        gate = jnp.zeros((chunk_rows, wg.shape[1]), F32)
        up = jnp.zeros((chunk_rows, wg.shape[1]), F32)
        for q in range(nx):
            rows_q = arr[q, c]
            gate = gate + dot(rows_q, wg[q * quarter : (q + 1) * quarter, :])
            up = up + dot(rows_q, wu[q * quarter : (q + 1) * quarter, :])
        hidden = (gate * jax.nn.sigmoid(gate) * up).astype(BF16)
        for q in range(nx):
            part[q, c] = dot(hidden, wd[:, q * quarter : (q + 1) * quarter]).astype(BF16)
        half_sends(c)
        quarter_sends(c)

    def flash_planes(first, end):
        @pl.loop(first, end)
        def _(d):
            zs = z - d
            for i, line_y in enumerate((y, y_down, y_up, y_far)):
                await_bytes(kv.at[zs, line_y * 2 + 1 - core], ks_recv.at[i, d])

            @pl.loop(0, jnp.where(d == 0, k_own // 2, nk // 2))
            def _(p):
                visit(zs, p, False)

            @pl.when(d == 0)
            def _():
                visit(zs, k_own // 2, True)

    near_step = nz // 2 + 1
    each = max(1, 2 * nx // nz)

    def planes(turn):
        mid = nz // 2
        first = turn - 1 + jnp.where(turn > mid, 1, 0)
        end = turn + jnp.where(turn >= mid, 1, 0) + jnp.where(turn > mid + 1, 1, 0)
        return first, jnp.minimum(end, z + 1)

    last_turn = nz // 2 + nz // 4

    @pl.loop(0, nz)
    def _(step):
        @pl.when(step >= 3)
        def _():
            pass_sums(step - 2)


        @pl.when(step >= 4)
        def _():
            finish(step - 3)


        @pl.when(step >= 2)
        def _():
            c = step - 1

            @pl.when(c == 1)
            def _():
                for load in loads[:3]:
                    load.wait()

            await_bytes(arr.at[far, c, low], fw_recv.at[0, c])
            await_bytes(arr.at[far, c, high], fw_recv.at[1, c])
            multiply(c)

        @pl.when((step >= 1) & (step < nz - 1))
        def _():
            c = step
            await_bytes(arr.at[left, c], ag_recv.at[0, c])
            send(arr.at[left, c, low], arr.at[left, c, low], fw_send.at[0, c], fw_recv.at[0, c], right)
            await_bytes(arr.at[right, c], ag_recv.at[1, c])
            send(arr.at[right, c, high], arr.at[right, c, high], fw_send.at[1, c], fw_recv.at[1, c], left)

        @pl.when(step == near_step)
        def _():
            await_bytes(arr.at[:, 0, first_rows], a2a_recv.at[0])
            multiply(0)

        @pl.when((step >= 2) & (step <= last_turn + 1))
        def _():
            @pl.loop(*planes(step - 1))
            def _(d):
                zs = z - d
                opposite = y_far * 2 + core
                await_bytes(kv.at[zs, opposite, b_low], kf_recv.at[0, d])
                await_bytes(kv.at[zs, opposite, b_high], kf_recv.at[1, d])
                send_block(kv.at[zs, opposite], ks_send.at[3, d], ks_recv.at[3, d], sibling)

        @pl.when((step >= 1) & (step <= last_turn))
        def _():
            @pl.loop(step, jnp.minimum(jnp.where(step == last_turn, nz, step + 1), z + 1))
            def _(d):
                await_bytes(kv.at[z - d, k_own], kz_recv.at[d])
                spread_column(d)

        @pl.when((step >= 1) & (step <= last_turn))
        def _():
            @pl.loop(*planes(step))
            def _(d):
                zs = z - d
                below = kv.at[zs, y_down * 2 + core]
                await_bytes(below, ky_recv.at[0, d])
                part_low = kv.at[zs, y_down * 2 + core, b_low]
                send_block(part_low, kf_send.at[0, d], kf_recv.at[0, d], up_dev)
                send_block(below, ks_send.at[1, d], ks_recv.at[1, d], sibling)
                above = kv.at[zs, y_up * 2 + core]
                await_bytes(above, ky_recv.at[1, d])
                part_high = kv.at[zs, y_up * 2 + core, b_high]
                send_block(part_high, kf_send.at[1, d], kf_recv.at[1, d], down_dev)
                send_block(above, ks_send.at[2, d], ks_recv.at[2, d], sibling)

        @pl.when(step + AHEAD + 1 < nz - 1)
        def _():
            prepare(step + AHEAD + 1)
            dispatch(step + AHEAD + 1)

        @pl.when((step >= 1) & (step <= nx // each))
        def _():
            @pl.loop((step - 1) * each, step * each)
            def _(q):
                dispatch_wide(0, q, 0, z)

        @pl.when((step >= 2) & (step <= nx // each + 1))
        def _():
            @pl.loop((step - 2) * each, (step - 1) * each)
            def _(q):
                dispatch_wide(1, q, nz - 1, below_z)

        @pl.when(step == near_step + 1)
        def _():
            pass_sums(0)

        @pl.when(step == near_step + 2)
        def _():
            finish(0)

        @pl.when(step == nz - 1)
        def _():
            await_bytes(arr.at[:, nz - 1], a2a_recv.at[nz - 1])
            multiply(nz - 1)

        @pl.when((step >= 2) & (step <= last_turn + 1))
        def _():
            first, end = planes(step - 1)
            flash_planes(first, jnp.where(step == nz - 1, jnp.minimum(first + 1, end), end))

        @pl.when(step == nz - 1)
        def _():
            pass_sums(nz - 2)
            finish(nz - 3)
            flash_planes(nz - 1, z + 1)

        @pl.when(step < nz - 3)
        def _():
            @pl.loop(jnp.where(step == 0, 1, step + 2), step + 3)
            def _(c):
                await_bytes(arr.at[x, c], a2a_recv.at[c])
                send(arr.at[x, c], arr.at[x, c], ag_send.at[0, c], ag_recv.at[0, c], right)
                send(arr.at[x, c], arr.at[x, c], ag_send.at[1, c], ag_recv.at[1, c], left)

    loads[3].wait()
    for h in range(heads):
        heads_ref[:, h * HD : (h + 1) * HD] = (acc_ref[h] / l_ref[h]).astype(BF16)
    for n in range(nx):
        mixed = dot(heads_ref[...], wo[:, n * quarter : (n + 1) * quarter]).astype(BF16)
        for q in range(nx):
            part[q, nz + n // 2, n % 2 * half : n % 2 * half + half, :] = mixed[
                q * half : (q + 1) * half, :
            ]
    pass_sums(nz - 1)
    half_sends(nz)
    half_sends(nz + 1)
    quarter_sends(nz)
    quarter_sends(nz + 1)
    finish(nz - 2)
    finish(nz - 1)

    @pl.loop(nz, nz + 2)
    def _(c):
        pass_sums(c)

    @pl.loop(nz, nz + 2)
    def _(c):
        finish(c)

    for n in range(nx):
        mixed_ref[:, n * quarter : (n + 1) * quarter] = part[
            x, nz + n // 2, n % 2 * half : n % 2 * half + half, :
        ]

    ret[slot_rows(e), :] = part[x, 0, slot_rows(k_own), :]
    await_bytes(ret.at[pl.ds(0, (n_ep - 1) * CAP)], ret_recv)
    o_ref[...] = (dot(c_hi[...], ret[...]) + dot(c_lo[...], ret[...])).astype(BF16)

    await_bytes(part.at[x, 0, first_rows], ret_send.at[0])
    await_bytes(part.at[x, nz - 1], ret_send.at[nz - 1])
    await_bytes(arr.at[:, nz - 1], a2a_send.at[nz - 1])
    await_bytes(arr.at[:, 0, first_rows], a2a_send.at[0])

    @pl.loop(1, nz - 1)
    def _(c):
        await_bytes(part.at[x, c], ret_send.at[c])
        await_bytes(arr.at[0, c], a2a_send.at[c])

    @pl.loop(0, nz)
    def _(c):
        @pl.when((c > 0) & (c < nz - 1))
        def _():
            for side in (0, 1):
                await_bytes(arr.at[0, c], ag_send.at[side, c])
                await_bytes(half_in.at[side, c], fw_send.at[side, c])

        @pl.when(c <= z)
        def _():
            block = kv.at[0, 0]

            @pl.when(z + 1 < nz)
            def _():
                await_bytes(block, kz_send.at[c])

            for side in (0, 1):
                await_bytes(block, ky_send.at[side, c])
                await_bytes(kv.at[0, 0, b_low], kf_send.at[side, c])
            for i in range(4):
                await_bytes(block, ks_send.at[i, c])

    @pl.loop(0, nz + 2)
    def _(c):
        for side in (0, 1):
            for sem in (hs_send, qa_send, qb_send):
                await_bytes(half_in.at[side, c], sem.at[side, c])


def per_device(
    queries, keys, values, cum_gates, out_proj,
    tokens, norm_gain, routes, route_weights, w_gate, w_up, w_down,
):
    rows, width = tokens.shape
    q_rows = queries.shape[0]
    heads = cum_gates.shape[1]
    n_ep, nx = lax.axis_size("ep"), lax.axis_size("tp")
    nk = NYC
    nz = n_ep // nk
    quarter = width // nx
    hidden = w_gate.shape[2]
    chunk = nk * CAP
    slots = n_ep * CAP
    block_rows = 2 * q_rows + 4 * (heads * q_rows // 128)
    vmem = pl.BlockSpec(memory_space=pltpu.VMEM)
    anywhere = pl.BlockSpec(memory_space=pl.ANY)
    dma = pltpu.SemaphoreType.DMA
    pair = dma((2, nz))
    more = dma((2, nz + 2))
    line = dma((nz + 1,))
    return pl.pallas_call(
        functools.partial(step_kernel, nz, nk, nx),
        out_shape=(
            jax.ShapeDtypeStruct((q_rows // nx, width), BF16),
            jax.ShapeDtypeStruct((rows, quarter), BF16),
        ),
        in_specs=[vmem] * 6 + [anywhere] * 6,
        out_specs=(vmem, vmem),
        scratch_shapes=[
            pltpu.VMEM((width, hidden), BF16),
            pltpu.VMEM((width, hidden), BF16),
            pltpu.VMEM((hidden, width), BF16),
            pltpu.VMEM(out_proj.shape, BF16),
            pltpu.VMEM((slots, quarter), BF16),
            pltpu.VMEM((nx, nz, chunk, quarter), BF16),
            pltpu.VMEM((nx, nz + 2, chunk, quarter), BF16),
            pltpu.VMEM((2, nz + 2, chunk // 2, quarter), BF16),
            pltpu.VMEM((2, nz + 2, chunk, quarter), BF16),
            pltpu.VMEM((slots, quarter), BF16),
            pltpu.VMEM((rows, slots), BF16),
            pltpu.VMEM((rows, slots), BF16),
            pltpu.VMEM((nz, nk, block_rows, HD), BF16),
            pltpu.VMEM((heads, q_rows, 1), F32),
            pltpu.VMEM((heads, q_rows, 1), F32),
            pltpu.VMEM((heads, q_rows, HD), F32),
            pltpu.VMEM((q_rows, heads * HD), BF16),
            pltpu.VMEM((rows, width), BF16),
            pltpu.VMEM((2, nx, chunk, quarter), BF16),
            dma((6,)),
            dma((nz,)), dma((nz,)),
            pair, pair, pair, pair,
            more, more, more, more, more, more,
            dma((nz,)),
            dma,
            line, line, pair, pair, pair, pair, dma((4, nz)), dma((4, nz)),
        ],
        compiler_params=pltpu.CompilerParams(
            collective_id=0, has_side_effects=True, vmem_limit_bytes=67043328
        ),
        cost_estimate=pl.CostEstimate(
            flops=100 * 10**9, bytes_accessed=10 * 2**20, transcendentals=0
        ),
    )(
        tokens, norm_gain[None], routes.T, route_weights.T, queries, cum_gates.T,
        w_gate[0], w_up[0], w_down[0], out_proj, keys, values,
    )


def solution(mesh):
    placed = (
        P("ep", "tp"), P("ep", "tp"), P("ep", "tp"), P("ep", "tp"), P("tp", None),
        P("ep", None), P(), P("ep", None), P("ep", None),
        P("ep", None, "tp"), P("ep", None, "tp"), P("ep", "tp", None),
    )
    return jax.shard_map(
        per_device,
        mesh=mesh,
        in_specs=placed,
        out_specs=(P(("ep", "tp"), None), P("ep", "tp")),
        check_vma=False,
    )
```

```python
import functools
import math

import jax
import jax.numpy as jnp
from jax import lax
from jax.experimental import pallas as pl
from jax.experimental.pallas import tpu as pltpu
from jax.sharding import PartitionSpec as P

HD = 128
CAP = 16
NYC = 8
LOG2E = math.log2(math.e)
MESH = pl.DeviceIdType.MESH
F32 = jnp.float32
BF16 = jnp.bfloat16
FLOOR = -1e30
AHEAD = 3


def iota(shape, dim):
    return lax.broadcasted_iota(jnp.int32, shape, dim)


def dot(a, b):
    return jnp.dot(a, b, preferred_element_type=F32)


def step_kernel(
    nz, nk, nx,
    tok_ref, gain_ref, routes_ref, rw_ref, q_ref, gates_ref,
    wg_hbm, wu_hbm, wd_hbm, wo_hbm, key_hbm, value_hbm,
    mixed_ref, o_ref,
    wg, wu, wd, wo, out, arr, part, half_in, quart_in, ret, c_hi, c_lo,
    kv, m_ref, l_ref, acc_ref, heads_ref, norm_ref, wide,
    w_sem, a2a_send, a2a_recv, ag_send, ag_recv, fw_send, fw_recv,
    hs_send, hs_recv, qa_send, qa_recv, qb_send, qb_recv, ret_send, ret_recv,
    kz_send, kz_recv, ky_send, ky_recv, kf_send, kf_recv, ks_send, ks_recv,
):
    e = lax.axis_index("ep")
    x = lax.axis_index("tp")
    n_ep = nz * nk
    ny = nk // 2
    z, k_own = e // nk, e % nk
    y, core = k_own // 2, k_own % 2
    right, left, far = (x + 1) % nx, (x + nx - 1) % nx, (x + 2) % nx
    rows, width = tok_ref.shape
    quarter = width // nx
    chunk_rows = nk * CAP
    half = chunk_rows // 2
    q_rows = q_ref.shape[0]
    heads = q_ref.shape[1] // HD
    block_rows = kv.shape[2]

    barrier = pltpu.get_barrier_semaphore()

    @pl.loop(1, n_ep)
    def _(k):
        pl.semaphore_signal(barrier, inc=1, device_id=((e + k) % n_ep, x), device_id_type=MESH)

    for side in (left, right):
        pl.semaphore_signal(barrier, inc=1, device_id=(e, side), device_id_type=MESH)

    own_kv = [
        pltpu.make_async_copy(key_hbm, kv.at[z, k_own, pl.ds(0, q_rows)], w_sem.at[4]),
        pltpu.make_async_copy(value_hbm, kv.at[z, k_own, pl.ds(q_rows, q_rows)], w_sem.at[5]),
    ]
    loads = [
        pltpu.make_async_copy(src, dst, w_sem.at[i])
        for i, (src, dst) in enumerate(((wg_hbm, wg), (wu_hbm, wu), (wd_hbm, wd), (wo_hbm, wo)))
    ]
    for load in own_kv + loads:
        load.start()

    lines = jnp.concatenate(
        [
            gates_ref[h : h + 1, i * 128 : (i + 1) * 128]
            for h in range(heads)
            for i in range(q_rows // 128)
        ],
        axis=0,
    )
    g_hi = lines.astype(BF16)
    rest = lines - g_hi.astype(F32)
    g_mid = rest.astype(BF16)
    g_lo = (rest - g_mid.astype(F32)).astype(BF16)
    n_lines = lines.shape[0]
    kv[z, k_own, 2 * q_rows :, :] = jnp.concatenate(
        [g_hi.astype(F32), g_mid.astype(F32), g_lo.astype(F32), jnp.zeros_like(lines)], axis=0
    ).astype(BF16)

    routes = routes_ref[...]
    e_row = iota((n_ep, rows), 0)
    named = jnp.zeros((n_ep, rows), F32)
    weight = jnp.zeros((n_ep, rows), F32)
    for k in range(routes.shape[0]):
        hit = routes[k : k + 1, :] == e_row
        named = named + hit.astype(F32)
        weight = weight + jnp.where(hit, rw_ref[k : k + 1, :], 0.0)
    before = (iota((rows, rows), 0) < iota((rows, rows), 1)).astype(BF16)
    named = named.astype(BF16)
    rank = dot(named, before).astype(BF16)

    tokens = tok_ref[...].astype(F32)
    inv = lax.rsqrt(jnp.mean(tokens * tokens, axis=-1, keepdims=True) + 1e-06)
    norm_ref[...] = (tokens * inv * gain_ref[...]).astype(BF16)
    normed = norm_ref[:, pl.ds(pl.multiple_of(x * quarter, quarter), quarter)]

    def picks(base):
        slot = iota((chunk_rows, n_ep), 0) + base
        spread = ((slot // CAP) == iota((chunk_rows, n_ep), 1)).astype(BF16)
        hit = (dot(spread, named) > 0.5) & (
            dot(spread, rank) == ((iota((chunk_rows, rows), 0) + base) % CAP).astype(F32)
        )
        return hit.astype(BF16)

    middle = [nz // 2]
    for near in range(2, (nz + 1) // 2):
        middle += [nz - near, near]
    order = [0, 1] + middle[1:] + middle[:1] + [nz - 1]

    def dz_of(c):
        return sum(jnp.where(c == i, dz, 0) for i, dz in enumerate(order))

    def prepare(c):
        base = (z + dz_of(c)) % nz * chunk_rows
        at = pl.ds(pl.multiple_of(base, chunk_rows), chunk_rows)
        out[at, :] = dot(picks(base), normed).astype(BF16)

    prepare(1)

    for load in own_kv:
        load.wait()
    pl.semaphore_wait(barrier, n_ep - 1 + 2)

    def slot_rows(index):
        return pl.ds(pl.multiple_of(index * CAP, CAP), CAP)

    def await_bytes(ref, sem):
        pltpu.make_async_copy(ref, ref, sem).wait()

    def send(src, dst, send_sem, recv_sem, to):
        pltpu.make_async_remote_copy(
            src, dst, send_sem, recv_sem, device_id=(e, to), device_id_type=MESH
        ).start()

    def send_block(ref, send_sem, recv_sem, to):
        pltpu.make_async_remote_copy(
            ref, ref, send_sem, recv_sem, device_id=(to, x), device_id_type=MESH
        ).start()

    def dispatch(c):
        dest_z = (z + dz_of(c)) % nz

        @pl.loop(0, nk)
        def _(k):
            dest = dest_z * nk + (k_own + k) % nk
            pltpu.make_async_remote_copy(
                out.at[slot_rows(dest)],
                arr.at[x, c, slot_rows(k_own)],
                a2a_send.at[c],
                a2a_recv.at[c],
                device_id=(dest, x),
                device_id_type=MESH,
            ).start()

    b_low, b_high = pl.ds(0, block_rows // 2), pl.ds(block_rows // 2, block_rows // 2)
    y_up, y_down, y_far = (y + 1) % ny, (y + ny - 1) % ny, (y + 2) % ny
    plane = z * nk
    up_dev, down_dev = plane + y_up * 2 + core, plane + y_down * 2 + core
    sibling = plane + y * 2 + (1 - core)

    def spread_column(d):
        block = kv.at[z - d, k_own]

        @pl.when(z + 1 < nz)
        def _():
            send_block(block, kz_send.at[d], kz_recv.at[d + 1], e + nk)

        send_block(block, ky_send.at[0, d], ky_recv.at[0, d], up_dev)
        send_block(block, ky_send.at[1, d], ky_recv.at[1, d], down_dev)
        send_block(block, ks_send.at[0, d], ks_recv.at[0, d], sibling)

    dispatch(1)
    spread_column(0)

    @pl.loop(2, min(AHEAD, nz - 2) + 1)
    def _(c):
        prepare(c)
        dispatch(c)

    below_z = (z + nz - 1) % nz
    for i, to_z in enumerate((z, below_z)):
        near = picks(to_z * chunk_rows)
        for q in range(nx):
            wide[i, q] = dot(near, norm_ref[:, q * quarter : (q + 1) * quarter]).astype(BF16)

    def dispatch_wide(i, q, c, to_z):
        @pl.loop(1 - i, nk)
        def _(k):
            k_dest = (k_own + k) % nk
            pltpu.make_async_remote_copy(
                wide.at[i, q, slot_rows(k_dest)],
                arr.at[q, c, slot_rows(k_own)],
                a2a_send.at[c],
                a2a_recv.at[c],
                device_id=(to_z * nk + k_dest, x),
                device_id_type=MESH,
            ).start()

    arr[:, 0, slot_rows(k_own), :] = wide[0, :, slot_rows(k_own), :]

    same = (iota((rows, rows), 0) == iota((rows, rows), 1)).astype(BF16)

    def turned(a):
        return lax.dot_general(
            same, a, (((1,), (1,)), ((), ())), preferred_element_type=F32
        ).astype(BF16)

    w_hi = weight.astype(BF16)
    w_lo = (weight - w_hi.astype(F32)).astype(BF16)
    slot = iota((n_ep, n_ep * CAP), 1)
    spread = ((slot // CAP) == iota((n_ep, n_ep * CAP), 0)).astype(BF16)
    keep = (dot(turned(named), spread) > 0.5) & (
        dot(turned(rank), spread) == (iota((rows, n_ep * CAP), 1) % CAP).astype(F32)
    )
    c_hi[...] = jnp.where(keep, dot(turned(w_hi), spread), 0.0).astype(BF16)
    c_lo[...] = jnp.where(keep, dot(turned(w_lo), spread), 0.0).astype(BF16)

    m_ref[...] = jnp.full_like(m_ref, FLOOR)
    l_ref[...] = jnp.zeros_like(l_ref)
    acc_ref[...] = jnp.zeros_like(acc_ref)
    halves = q_rows // 128
    ratio = HD ** (-0.5) * LOG2E

    def visit(zs, p, masked):
        both = pl.ds(2 * p, 2)
        key = kv[zs, both, 0:q_rows, :].reshape(2 * q_rows, HD)
        value = kv[zs, both, q_rows : 2 * q_rows, :].reshape(2 * q_rows, HD)
        terms = kv[zs, both, 2 * q_rows :, :].astype(F32)
        n = n_lines
        gates = terms[:, 0:n] + terms[:, n : 2 * n] + terms[:, 2 * n : 3 * n]
        if masked:
            pos = p * 2 * q_rows + iota((q_rows, 2 * q_rows), 1)
            own_pos = k_own * q_rows + iota((q_rows, 2 * q_rows), 0)
            allowed = pos <= own_pos
        for h in range(heads):
            line = jnp.concatenate(
                [gates[b, h * halves + i : h * halves + i + 1, :] for b in range(2) for i in range(halves)],
                axis=1,
            )
            line = (line - gates_ref[h : h + 1, 0:1]) * LOG2E
            s = lax.dot_general(
                q_ref[:, h * HD : (h + 1) * HD], key, (((1,), (1,)), ((), ())), preferred_element_type=F32
            )
            t = s * ratio - line
            if masked:
                t = jnp.where(allowed, t, FLOOR)
            old = m_ref[h]
            new = jnp.maximum(old, jnp.max(t, axis=1, keepdims=True))
            alpha = jnp.exp2(old - new)
            w = jnp.exp2(t - new)
            l_ref[h] = alpha * l_ref[h] + jnp.sum(w, axis=1, keepdims=True)
            acc_ref[h] = alpha * acc_ref[h] + dot(w.astype(BF16), value)
            m_ref[h] = new

    low, high = pl.ds(0, half), pl.ds(half, half)
    first_rows = pl.ds(0, (nk - 1) * CAP)
    def half_sends(c):
        send(part.at[far, c, low], half_in.at[0, c], hs_send.at[0, c], hs_recv.at[0, c], right)
        send(part.at[far, c, high], half_in.at[1, c], hs_send.at[1, c], hs_recv.at[1, c], left)

    def quarter_sends(c):
        send(part.at[right, c, high], quart_in.at[0, c, high], qa_send.at[0, c], qa_recv.at[0, c], right)
        send(part.at[left, c, low], quart_in.at[1, c, low], qa_send.at[1, c], qa_recv.at[1, c], left)

    def pass_sums(c):
        await_bytes(half_in.at[0, c], hs_recv.at[0, c])
        part[right, c, 0:half, :] = (
            part[right, c, 0:half, :].astype(F32) + half_in[0, c].astype(F32)
        ).astype(BF16)
        send(part.at[right, c, low], quart_in.at[0, c, low], qb_send.at[0, c], qb_recv.at[0, c], right)
        await_bytes(half_in.at[1, c], hs_recv.at[1, c])
        part[left, c, half:, :] = (
            part[left, c, half:, :].astype(F32) + half_in[1, c].astype(F32)
        ).astype(BF16)
        send(part.at[left, c, high], quart_in.at[1, c, high], qb_send.at[1, c], qb_recv.at[1, c], left)

    def finish(c):
        await_bytes(quart_in.at[0, c, high], qa_recv.at[0, c])
        await_bytes(quart_in.at[1, c, low], qa_recv.at[1, c])
        await_bytes(quart_in.at[0, c, low], qb_recv.at[0, c])
        await_bytes(quart_in.at[1, c, high], qb_recv.at[1, c])
        part[x, c] = (
            part[x, c].astype(F32) + quart_in[0, c].astype(F32) + quart_in[1, c].astype(F32)
        ).astype(BF16)

        @pl.when(c < nz)
        def _():
            home_z = (z + nz - dz_of(c)) % nz

            @pl.loop(jnp.where(c == 0, 1, 0), nk)
            def _(k):
                k_home = (k_own + k) % nk
                pltpu.make_async_remote_copy(
                    part.at[x, c, slot_rows(k_home)],
                    ret.at[slot_rows(e)],
                    ret_send.at[c],
                    ret_recv,
                    device_id=(home_z * nk + k_home, x),
                    device_id_type=MESH,
                ).start()

    def multiply(c):
        gate = jnp.zeros((chunk_rows, wg.shape[1]), F32)
        up = jnp.zeros((chunk_rows, wg.shape[1]), F32)
        for q in range(nx):
            rows_q = arr[q, c]
            gate = gate + dot(rows_q, wg[q * quarter : (q + 1) * quarter, :])
            up = up + dot(rows_q, wu[q * quarter : (q + 1) * quarter, :])
        hidden = (gate * jax.nn.sigmoid(gate) * up).astype(BF16)
        for q in range(nx):
            part[q, c] = dot(hidden, wd[:, q * quarter : (q + 1) * quarter]).astype(BF16)
        half_sends(c)
        quarter_sends(c)

    def flash_planes(first, end):
        @pl.loop(first, end)
        def _(d):
            zs = z - d
            for i, line_y in enumerate((y, y_down, y_up, y_far)):
                await_bytes(kv.at[zs, line_y * 2 + 1 - core], ks_recv.at[i, d])

            @pl.loop(0, jnp.where(d == 0, k_own // 2, nk // 2))
            def _(p):
                visit(zs, p, False)

            @pl.when(d == 0)
            def _():
                visit(zs, k_own // 2, True)

    near_step = nz // 2 + 1
    each = max(1, 2 * nx // nz)

    def planes(turn):
        mid = nz // 2
        first = turn - 1 + jnp.where(turn > mid, 1, 0)
        end = turn + jnp.where(turn >= mid, 1, 0) + jnp.where(turn > mid + 1, 1, 0)
        return first, jnp.minimum(end, z + 1)

    last_turn = nz // 2 + nz // 4

    @pl.loop(0, nz)
    def _(step):
        @pl.when(step >= 3)
        def _():
            pass_sums(step - 2)


        @pl.when(step >= 4)
        def _():
            finish(step - 3)


        @pl.when(step >= 2)
        def _():
            c = step - 1

            @pl.when(c == 1)
            def _():
                for load in loads[:3]:
                    load.wait()

            await_bytes(arr.at[far, c, low], fw_recv.at[0, c])
            await_bytes(arr.at[far, c, high], fw_recv.at[1, c])
            multiply(c)

        @pl.when((step >= 1) & (step < nz - 1))
        def _():
            c = step
            await_bytes(arr.at[left, c], ag_recv.at[0, c])
            send(arr.at[left, c, low], arr.at[left, c, low], fw_send.at[0, c], fw_recv.at[0, c], right)
            await_bytes(arr.at[right, c], ag_recv.at[1, c])
            send(arr.at[right, c, high], arr.at[right, c, high], fw_send.at[1, c], fw_recv.at[1, c], left)

        @pl.when(step == near_step)
        def _():
            await_bytes(arr.at[:, 0, first_rows], a2a_recv.at[0])
            multiply(0)

        @pl.when((step >= 2) & (step <= last_turn + 1))
        def _():
            @pl.loop(*planes(step - 1))
            def _(d):
                zs = z - d
                opposite = y_far * 2 + core
                await_bytes(kv.at[zs, opposite, b_low], kf_recv.at[0, d])
                await_bytes(kv.at[zs, opposite, b_high], kf_recv.at[1, d])
                send_block(kv.at[zs, opposite], ks_send.at[3, d], ks_recv.at[3, d], sibling)

        @pl.when((step >= 1) & (step <= last_turn))
        def _():
            @pl.loop(step, jnp.minimum(jnp.where(step == last_turn, nz, step + 1), z + 1))
            def _(d):
                await_bytes(kv.at[z - d, k_own], kz_recv.at[d])
                spread_column(d)

        @pl.when((step >= 1) & (step <= last_turn))
        def _():
            @pl.loop(*planes(step))
            def _(d):
                zs = z - d
                below = kv.at[zs, y_down * 2 + core]
                await_bytes(below, ky_recv.at[0, d])
                part_low = kv.at[zs, y_down * 2 + core, b_low]
                send_block(part_low, kf_send.at[0, d], kf_recv.at[0, d], up_dev)
                send_block(below, ks_send.at[1, d], ks_recv.at[1, d], sibling)
                above = kv.at[zs, y_up * 2 + core]
                await_bytes(above, ky_recv.at[1, d])
                part_high = kv.at[zs, y_up * 2 + core, b_high]
                send_block(part_high, kf_send.at[1, d], kf_recv.at[1, d], down_dev)
                send_block(above, ks_send.at[2, d], ks_recv.at[2, d], sibling)

        @pl.when(step + AHEAD + 1 < nz - 1)
        def _():
            prepare(step + AHEAD + 1)
            dispatch(step + AHEAD + 1)

        @pl.when((step >= 1) & (step <= nx // each))
        def _():
            @pl.loop((step - 1) * each, step * each)
            def _(q):
                dispatch_wide(0, q, 0, z)

        @pl.when((step >= 2) & (step <= nx // each + 1))
        def _():
            @pl.loop((step - 2) * each, (step - 1) * each)
            def _(q):
                dispatch_wide(1, q, nz - 1, below_z)

        @pl.when(step == near_step + 1)
        def _():
            pass_sums(0)

        @pl.when(step == near_step + 2)
        def _():
            finish(0)

        @pl.when(step == nz - 1)
        def _():
            await_bytes(arr.at[:, nz - 1], a2a_recv.at[nz - 1])
            multiply(nz - 1)

        @pl.when((step >= 2) & (step <= last_turn + 1))
        def _():
            first, end = planes(step - 1)
            flash_planes(first, jnp.where(step == nz - 1, jnp.minimum(first + 1, end), end))

        @pl.when(step == nz - 1)
        def _():
            pass_sums(nz - 2)
            finish(nz - 3)
            flash_planes(nz - 1, z + 1)

        @pl.when(step < nz - 3)
        def _():
            @pl.loop(jnp.where(step == 0, 1, step + 2), step + 3)
            def _(c):
                await_bytes(arr.at[x, c], a2a_recv.at[c])
                send(arr.at[x, c], arr.at[x, c], ag_send.at[0, c], ag_recv.at[0, c], right)
                send(arr.at[x, c], arr.at[x, c], ag_send.at[1, c], ag_recv.at[1, c], left)

    loads[3].wait()
    for h in range(heads):
        heads_ref[:, h * HD : (h + 1) * HD] = (acc_ref[h] / l_ref[h]).astype(BF16)
    for n in range(nx):
        mixed = dot(heads_ref[...], wo[:, n * quarter : (n + 1) * quarter]).astype(BF16)
        for q in range(nx):
            part[q, nz + n // 2, n % 2 * half : n % 2 * half + half, :] = mixed[
                q * half : (q + 1) * half, :
            ]
    pass_sums(nz - 1)
    half_sends(nz)
    half_sends(nz + 1)
    quarter_sends(nz)
    quarter_sends(nz + 1)
    finish(nz - 2)
    finish(nz - 1)

    @pl.loop(nz, nz + 2)
    def _(c):
        pass_sums(c)

    @pl.loop(nz, nz + 2)
    def _(c):
        finish(c)

    for n in range(nx):
        mixed_ref[:, n * quarter : (n + 1) * quarter] = part[
            x, nz + n // 2, n % 2 * half : n % 2 * half + half, :
        ]

    ret[slot_rows(e), :] = part[x, 0, slot_rows(k_own), :]
    await_bytes(ret.at[pl.ds(0, (n_ep - 1) * CAP)], ret_recv)
    o_ref[...] = (dot(c_hi[...], ret[...]) + dot(c_lo[...], ret[...])).astype(BF16)

    await_bytes(part.at[x, 0, first_rows], ret_send.at[0])
    await_bytes(part.at[x, nz - 1], ret_send.at[nz - 1])
    await_bytes(arr.at[:, nz - 1], a2a_send.at[nz - 1])
    await_bytes(arr.at[:, 0, first_rows], a2a_send.at[0])

    @pl.loop(1, nz - 1)
    def _(c):
        await_bytes(part.at[x, c], ret_send.at[c])
        await_bytes(arr.at[0, c], a2a_send.at[c])

    @pl.loop(0, nz)
    def _(c):
        @pl.when((c > 0) & (c < nz - 1))
        def _():
            for side in (0, 1):
                await_bytes(arr.at[0, c], ag_send.at[side, c])
                await_bytes(half_in.at[side, c], fw_send.at[side, c])

        @pl.when(c <= z)
        def _():
            block = kv.at[0, 0]

            @pl.when(z + 1 < nz)
            def _():
                await_bytes(block, kz_send.at[c])

            for side in (0, 1):
                await_bytes(block, ky_send.at[side, c])
                await_bytes(kv.at[0, 0, b_low], kf_send.at[side, c])
            for i in range(4):
                await_bytes(block, ks_send.at[i, c])

    @pl.loop(0, nz + 2)
    def _(c):
        for side in (0, 1):
            for sem in (hs_send, qa_send, qb_send):
                await_bytes(half_in.at[side, c], sem.at[side, c])


def put_out(a_ref, b_ref, a_out, b_out):
    a_out[...] = a_ref[...]
    b_out[...] = b_ref[...]


def per_device(
    queries, keys, values, cum_gates, out_proj,
    tokens, norm_gain, routes, route_weights, w_gate, w_up, w_down,
):
    rows, width = tokens.shape
    q_rows = queries.shape[0]
    heads = cum_gates.shape[1]
    n_ep, nx = lax.axis_size("ep"), lax.axis_size("tp")
    nk = NYC
    nz = n_ep // nk
    quarter = width // nx
    hidden = w_gate.shape[2]
    chunk = nk * CAP
    slots = n_ep * CAP
    block_rows = 2 * q_rows + 4 * (heads * q_rows // 128)
    vmem = pl.BlockSpec(memory_space=pltpu.VMEM)
    anywhere = pl.BlockSpec(memory_space=pl.ANY)
    dma = pltpu.SemaphoreType.DMA
    pair = dma((2, nz))
    more = dma((2, nz + 2))
    line = dma((nz + 1,))
    results = pl.pallas_call(
        functools.partial(step_kernel, nz, nk, nx),
        out_shape=(
            jax.ShapeDtypeStruct((q_rows // nx, width), BF16),
            jax.ShapeDtypeStruct((rows, quarter), BF16),
        ),
        in_specs=[vmem] * 6 + [anywhere] * 6,
        out_specs=(vmem, vmem),
        scratch_shapes=[
            pltpu.VMEM((width, hidden), BF16),
            pltpu.VMEM((width, hidden), BF16),
            pltpu.VMEM((hidden, width), BF16),
            pltpu.VMEM(out_proj.shape, BF16),
            pltpu.VMEM((slots, quarter), BF16),
            pltpu.VMEM((nx, nz, chunk, quarter), BF16),
            pltpu.VMEM((nx, nz + 2, chunk, quarter), BF16),
            pltpu.VMEM((2, nz + 2, chunk // 2, quarter), BF16),
            pltpu.VMEM((2, nz + 2, chunk, quarter), BF16),
            pltpu.VMEM((slots, quarter), BF16),
            pltpu.VMEM((rows, slots), BF16),
            pltpu.VMEM((rows, slots), BF16),
            pltpu.VMEM((nz, nk, block_rows, HD), BF16),
            pltpu.VMEM((heads, q_rows, 1), F32),
            pltpu.VMEM((heads, q_rows, 1), F32),
            pltpu.VMEM((heads, q_rows, HD), F32),
            pltpu.VMEM((q_rows, heads * HD), BF16),
            pltpu.VMEM((rows, width), BF16),
            pltpu.VMEM((2, nx, chunk, quarter), BF16),
            dma((6,)),
            dma((nz,)), dma((nz,)),
            pair, pair, pair, pair,
            more, more, more, more, more, more,
            dma((nz,)),
            dma,
            line, line, pair, pair, pair, pair, dma((4, nz)), dma((4, nz)),
        ],
        compiler_params=pltpu.CompilerParams(
            collective_id=0, has_side_effects=True, vmem_limit_bytes=67043328
        ),
        cost_estimate=pl.CostEstimate(
            flops=100 * 10**9, bytes_accessed=10 * 2**20, transcendentals=0
        ),
    )(
        tokens, norm_gain[None], routes.T, route_weights.T, queries, cum_gates.T,
        w_gate[0], w_up[0], w_down[0], out_proj, keys, values,
    )
    return pl.pallas_call(
        put_out,
        out_shape=tuple(jax.ShapeDtypeStruct(r.shape, r.dtype) for r in results),
        in_specs=[vmem] * 2,
        out_specs=(vmem, vmem),
    )(*results)


def solution(mesh):
    placed = (
        P("ep", "tp"), P("ep", "tp"), P("ep", "tp"), P("ep", "tp"), P("tp", None),
        P("ep", None), P(), P("ep", None), P("ep", None),
        P("ep", None, "tp"), P("ep", None, "tp"), P("ep", "tp", None),
    )
    return jax.shard_map(
        per_device,
        mesh=mesh,
        in_specs=placed,
        out_specs=(P(("ep", "tp"), None), P("ep", "tp")),
        check_vma=False,
    )
```
